768 devices in a mesh: sp: 12 (over z), tp: 8 (over y), dp: 8 (over x, core).
Axes of the slice: x: 4, y: 8, z: 12, core: 2. Of those that a mesh axis runs over, the one named last changes fastest.
Arguments:
- latent: bfloat16 [30720, 3072], P(('dp', 'sp', 'tp')), parts along dimension 0, may hold values from -6 to 6
- condition: float32 [24576], P('dp'), parts along dimension 0, may hold values from -8 to 8
- ctx_condition: float32 [3072], replicated, may hold values from -8 to 8
- context: bfloat16 [3072, 3072], P(('dp', 'sp')), parts along dimension 0, may hold values from -6 to 6
- mod_shift: bfloat16 [3072, 3072], P('sp', 'tp'), may hold values from -0.109375 to 0.109375
- mod_scale: bfloat16 [3072, 3072], P('sp', 'tp'), may hold values from -0.109375 to 0.109375
- mod_gate: bfloat16 [3072, 3072], P('sp', 'tp'), may hold values from -0.109375 to 0.109375
- norm_gain: float32 [3072], replicated, may hold values from 0.5 to 6
- w_query: bfloat16 [3072, 3072], P(None, 'tp'), may hold values from -0.109375 to 0.109375
- key_weight: bfloat16 [3072, 512], P(None, 'tp'), may hold values from -0.109375 to 0.109375
- value_weight: bfloat16 [3072, 512], P(None, 'tp'), may hold values from -0.109375 to 0.109375
- w_gate: bfloat16 [3072, 3072], P(None, 'tp'), may hold values from -0.109375 to 0.109375
- w_out: bfloat16 [3072, 3072], P('tp'), may hold values from -1.5 to 1.5
- sink_logit: float32 [48], P('tp'), may hold values from 4 to 7.5
Outputs:
- updated_latent: bfloat16 [30720, 3072], P(('dp', 'sp', 'tp')), parts along dimension 0
The draws below stay inside these ranges and needn't reach their ends.
There are 8 independent parts, one for each index of `dp`. The reference program is written for one: setup_inputs(seed, part) draws one part's arguments, and reference() takes and returns one part's arrays. A program takes and returns all parts, laid end to end along the dimension named above; an argument that names none is the same for every part. Nothing has to cross between parts.
All inputs are finite; a program needn't handle non-finite values.
Results may differ from the reference program's by a relative error of at most 0.02.
The reference program's roundings to bfloat16 on the way count: a program that leaves them out, or rounds other values in their place, can miss the bound.
Values may be sent and summed in bfloat16 or wider, within the bound.
No kernel may reach another device: no remote copies, remote signals or barrier semaphores. Data moves between devices by JAX's collectives and lax.ppermute only.
A program may use at most 64 MiB of HBM per device.

```python
import math
import jax
import jax.numpy as jnp
from jax import lax

MODEL_WIDTH = 3072
HEAD_SIZE = 64
HQ = 48
KEY_VALUE_HEADS = 8
L_DEV = 320
WINDOW = 128
GRID_W = 64
SEQ = 3840
CTX = 384
N_TP = 8


def draw_norm_gain(key, part):
    return jax.random.uniform(key, (MODEL_WIDTH,), jnp.float32, 0.5, 1.5)


def block_scale(own_key, extent, split, low, largest):
    gain, own = 1.0, jax.random.fold_in(own_key, 6)
    for axis_at, shards_of in split:
        draws = jnp.exp(jax.random.uniform(jax.random.fold_in(own, axis_at), (shards_of,), jnp.float32, low / len(split), largest / len(split)))
        gain = gain * jnp.repeat(draws, extent[axis_at] // shards_of).reshape([-1 if axis == axis_at else 1 for axis in range(len(extent))])
    return gain


def scatter_about(stream_key, shape, spread, most, cuts=(), held_as=jnp.bfloat16):
    gain = block_scale(stream_key, shape, cuts, -0.22, 0.18) if cuts else 1.0
    values = jax.random.normal(stream_key, shape, jnp.float32) * spread * gain
    return jnp.minimum(jnp.maximum(values, -most), most).astype(held_as)


def setup_inputs(seed: int = 0, part: int = 0) -> dict:
    streams_of = jax.random.split(jax.random.key(seed), 15)
    part_keys = jax.random.split(jax.random.fold_in(streams_of[14], part), 15)
    return {
        "latent": scatter_about(part_keys[0], (SEQ, MODEL_WIDTH), 1.0, 6.0, ((0, 96),)),
        "condition": scatter_about(part_keys[1], (MODEL_WIDTH,), 1.5, 8.0, (), jnp.float32),
        "ctx_condition": scatter_about(streams_of[2], (MODEL_WIDTH,), 1.5, 8.0, (), jnp.float32),
        "context": scatter_about(part_keys[3], (CTX, MODEL_WIDTH), 1.0, 6.0, ((0, 12),)),
        "mod_shift": scatter_about(streams_of[4], (MODEL_WIDTH, MODEL_WIDTH), MODEL_WIDTH ** -0.5, 0.109375, ((0, 12), (1, 8))),
        "mod_scale": scatter_about(streams_of[5], (MODEL_WIDTH, MODEL_WIDTH), MODEL_WIDTH ** -0.5, 0.109375, ((0, 12), (1, 8))),
        "mod_gate": scatter_about(streams_of[6], (MODEL_WIDTH, MODEL_WIDTH), MODEL_WIDTH ** -0.5, 0.109375, ((0, 12), (1, 8))),
        "norm_gain": draw_norm_gain(jax.random.fold_in(streams_of[14], 71), part),
        "w_query": scatter_about(streams_of[8], (MODEL_WIDTH, HQ * HEAD_SIZE), MODEL_WIDTH ** -0.5, 0.109375, ((1, 8),)),
        "key_weight": scatter_about(streams_of[9], (MODEL_WIDTH, KEY_VALUE_HEADS * HEAD_SIZE), MODEL_WIDTH ** -0.5, 0.109375, ((1, 8),)),
        "value_weight": scatter_about(streams_of[10], (MODEL_WIDTH, KEY_VALUE_HEADS * HEAD_SIZE), MODEL_WIDTH ** -0.5, 0.109375, ((1, 8),)),
        "w_gate": scatter_about(streams_of[11], (MODEL_WIDTH, HQ * HEAD_SIZE), MODEL_WIDTH ** -0.5, 0.109375, ((1, 8),)),
        "w_out": scatter_about(streams_of[12], (HQ * HEAD_SIZE, MODEL_WIDTH), 16 ** -0.5, 1.5, ((0, 8),)),
        "sink_logit": jnp.clip(4.0 + 3.5 * jax.random.uniform(streams_of[13], (HQ,), jnp.float32) ** block_scale(streams_of[13], (HQ,), ((0, 8),), -0.2, 0.2), 4.0, 7.5),
    }


NORM_EPS = 1e-06
MASK_VALUE = -1e+30

def modulate(row_data, gain_vec, shift_vec, scale_vec):
    values = row_data.astype(jnp.float32)
    inverse = lax.rsqrt(lax.optimization_barrier(jnp.mean(values * values, axis=-1, keepdims=True)) + NORM_EPS)
    return (values * inverse * gain_vec * (1.0 + scale_vec) + shift_vec).astype(jnp.bfloat16)

def rotate(projected, positions):
    row_count = projected.shape[0]
    head_count = projected.shape[1] // HEAD_SIZE
    quarter = HEAD_SIZE // 4
    half_dim = HEAD_SIZE // 2
    inverse = jnp.exp(-math.log(10000.0) * jnp.arange(quarter, dtype=jnp.float32) / quarter)
    grid_row = (positions // GRID_W).astype(jnp.float32)
    mesh_column = (positions % GRID_W).astype(jnp.float32)
    angles = jnp.concatenate([grid_row[:, None] * inverse, mesh_column[:, None] * inverse], axis=1)
    cosine = jnp.cos(angles)[:, None, :]
    sine_table = jnp.sin(angles)[:, None, :]
    shaped = projected.reshape(row_count, head_count, HEAD_SIZE)
    first_half = shaped[..., :half_dim]
    second = shaped[..., half_dim:]
    turned = jnp.concatenate([first_half * cosine - second * sine_table, second * cosine + first_half * sine_table], axis=-1)
    return turned.reshape(row_count, head_count * HEAD_SIZE)

def attend(queries, key_rows, value_rows, ctx_keys, ctx_values, sink_logit, q_begin, k_begin, seq_total):
    row_count = queries.shape[0]
    key_count = key_rows.shape[0]
    ctx_count = ctx_keys.shape[0]
    kv_heads = key_rows.shape[1] // HEAD_SIZE
    head_count = queries.shape[1] // HEAD_SIZE
    group_size = head_count // kv_heads
    factor = 1.0 / math.sqrt(HEAD_SIZE)
    q_heads = queries.astype(jnp.float32).reshape(row_count, kv_heads, group_size, HEAD_SIZE)
    k_heads = key_rows.astype(jnp.float32).reshape(key_count, kv_heads, HEAD_SIZE)
    v_heads = value_rows.astype(jnp.float32).reshape(key_count, kv_heads, HEAD_SIZE)
    ck_heads = ctx_keys.astype(jnp.float32).reshape(ctx_count, kv_heads, HEAD_SIZE)
    cv_heads = ctx_values.astype(jnp.float32).reshape(ctx_count, kv_heads, HEAD_SIZE)
    near_scores = jnp.einsum('qkgd,skd->kgqs', q_heads, k_heads) * factor
    q_pos = q_begin + jnp.arange(row_count, dtype=jnp.int32)
    k_pos = k_begin + jnp.arange(key_count, dtype=jnp.int32)
    in_window = (jnp.abs(q_pos[:, None] - k_pos[None, :]) <= WINDOW) & ((k_pos >= 0) & (k_pos < seq_total))[None, :]
    near_scores = jnp.where(in_window, near_scores, MASK_VALUE)
    ctx_scores = jnp.einsum('qkgd,skd->kgqs', q_heads, ck_heads) * factor
    sink_score = sink_logit.astype(jnp.float32).reshape(kv_heads, group_size)[:, :, None, None]
    peak_score = jnp.maximum(jnp.maximum(lax.optimization_barrier(jnp.max(near_scores, axis=-1, keepdims=True)), lax.optimization_barrier(jnp.max(ctx_scores, axis=-1, keepdims=True))), sink_score)
    near_exp = jnp.exp(near_scores - peak_score)
    ctx_exp = jnp.exp(ctx_scores - peak_score)
    softmax_denominator = lax.optimization_barrier(jnp.sum(near_exp, axis=-1, keepdims=True)) + lax.optimization_barrier(jnp.sum(ctx_exp, axis=-1, keepdims=True)) + jnp.exp(sink_score - peak_score)
    near_weights = (near_exp / softmax_denominator).astype(jnp.bfloat16)
    ctx_weights = (ctx_exp / softmax_denominator).astype(jnp.bfloat16)
    result = jnp.einsum('kgqs,skd->qkgd', near_weights.astype(jnp.float32), v_heads)
    result = result + jnp.einsum('kgqs,skd->qkgd', ctx_weights.astype(jnp.float32), cv_heads)
    return result.reshape(row_count, head_count * HEAD_SIZE)

def project_vec(vector, matrix):
    return jnp.dot(vector[None, :], matrix, preferred_element_type=jnp.float32)[0]

def reference(latent, condition, ctx_condition, context, mod_shift, mod_scale, mod_gate, norm_gain, w_query, key_weight, value_weight, w_gate, w_out, sink_logit):
    cond_act = jax.nn.silu(condition.astype(jnp.float32)).astype(jnp.bfloat16)
    ctx_act = jax.nn.silu(ctx_condition.astype(jnp.float32)).astype(jnp.bfloat16)
    lat_shift = project_vec(cond_act, mod_shift)
    lat_scale = project_vec(cond_act, mod_scale)
    lat_gate = project_vec(cond_act, mod_gate)
    ctx_shift = project_vec(ctx_act, mod_shift)
    ctx_scale = project_vec(ctx_act, mod_scale)
    hidden = modulate(latent, norm_gain, lat_shift, lat_scale)
    ctx_hidden = modulate(context, norm_gain, ctx_shift, ctx_scale)
    seq_total = latent.shape[0]
    positions = jnp.arange(seq_total, dtype=jnp.int32)
    queries = rotate(jnp.dot(hidden, w_query, preferred_element_type=jnp.float32), positions).astype(jnp.bfloat16)
    key_rows = rotate(jnp.dot(hidden, key_weight, preferred_element_type=jnp.float32), positions).astype(jnp.bfloat16)
    value_rows = jnp.dot(hidden, value_weight, preferred_element_type=jnp.float32).astype(jnp.bfloat16)
    gate_proj = jnp.dot(hidden, w_gate, preferred_element_type=jnp.float32).astype(jnp.bfloat16)
    ctx_keys = jnp.dot(ctx_hidden, key_weight, preferred_element_type=jnp.float32).astype(jnp.bfloat16)
    ctx_values = jnp.dot(ctx_hidden, value_weight, preferred_element_type=jnp.float32).astype(jnp.bfloat16)
    key_pad = jnp.pad(key_rows, ((WINDOW, WINDOW), (0, 0)))
    value_pad = jnp.pad(value_rows, ((WINDOW, WINDOW), (0, 0)))
    key_span = L_DEV + 2 * WINDOW

    def one_block(block_index):
        begin_row = (block_index * L_DEV).astype(jnp.int32)
        q_block = lax.dynamic_slice_in_dim(queries, begin_row, L_DEV, 0)
        k_block = lax.dynamic_slice_in_dim(key_pad, begin_row, key_span, 0)
        v_block = lax.dynamic_slice_in_dim(value_pad, begin_row, key_span, 0)
        return attend(q_block, k_block, v_block, ctx_keys, ctx_values, sink_logit, begin_row, begin_row - WINDOW, seq_total)
    blocks = lax.map(one_block, jnp.arange(seq_total // L_DEV, dtype=jnp.int32))
    attended = blocks.reshape(seq_total, queries.shape[1])
    mixed = (attended * jax.nn.silu(gate_proj.astype(jnp.float32))).astype(jnp.bfloat16)
    group_size = w_out.shape[0] // N_TP
    branch = jnp.zeros(latent.shape, jnp.float32)
    for group_index in range(N_TP):
        lower = group_index * group_size
        partial_term = jnp.dot(mixed[:, lower:lower + group_size], w_out[lower:lower + group_size], preferred_element_type=jnp.float32)
        branch = branch + lax.optimization_barrier(partial_term.astype(jnp.bfloat16)).astype(jnp.float32)
    return (latent.astype(jnp.float32) + lat_gate * branch).astype(jnp.bfloat16)
```

```python
import math

import jax
import jax.numpy as jnp
from jax import lax
from jax.sharding import PartitionSpec as P

HEAD_SIZE = 64
WINDOW = 128
GRID_W = 64


NORM_EPS = 1e-06
MASK_VALUE = -1e30


def copy_for_each(shard, axis):
    copies = jnp.broadcast_to(shard, (lax.axis_size(axis), *shard.shape))
    return lax.all_to_all(copies, axis, split_axis=0, concat_axis=0, tiled=True)


def taken_together(shard, axis):
    everything = copy_for_each(shard, axis)
    return jnp.sum(everything, axis=0)


def laid_out(tiles, dim):
    tiles = jnp.moveaxis(tiles, 0, dim)
    lengths = tiles.shape
    return tiles.reshape(*lengths[:dim], lengths[dim] * lengths[dim + 1], *lengths[dim + 2 :])


def gather_directly(shard, axis, dim):
    return laid_out(copy_for_each(shard, axis), dim)


def with_halo(block, sides, width):
    for axis, dim in sides:
        count = lax.axis_size(axis)
        forward = [(i, i + 1) for i in range(count - 1)]
        backward = [(target, source) for source, target in forward]
        low = lax.ppermute(
            lax.slice_in_dim(block, block.shape[dim] - width, None, axis=dim), axis, forward
        )
        high = lax.ppermute(lax.slice_in_dim(block, 0, width, axis=dim), axis, backward)
        block = jnp.concatenate([low, block, high], axis=dim)
    return block


def cut_along(shard, dim, size):
    before, after = (shard.shape[:dim], shard.shape[dim + 1 :])
    return jnp.moveaxis(shard.reshape(*before, size, -1, *after), dim, 0)


def sum_at_owner(shard, axis, dim):
    size = lax.axis_size(axis)
    tiles = lax.all_to_all(cut_along(shard, dim, size), axis, 0, 0, tiled=True)
    return jnp.sum(tiles.astype(jnp.float32), axis=0)


def modulate(row_data, gain_vec, shift_vec, scale_vec):
    values = row_data.astype(jnp.float32)
    inverse = lax.rsqrt(jnp.mean(values * values, axis=-1, keepdims=True) + NORM_EPS)
    return (values * inverse * gain_vec * (1.0 + scale_vec) + shift_vec).astype(jnp.bfloat16)


def rotate(projected, positions):
    row_count = projected.shape[0]
    head_count = projected.shape[1] // HEAD_SIZE
    quarter = HEAD_SIZE // 4
    half_dim = HEAD_SIZE // 2
    inverse = jnp.exp(-math.log(10000.0) * jnp.arange(quarter, dtype=jnp.float32) / quarter)
    grid_row = (positions // GRID_W).astype(jnp.float32)
    mesh_column = (positions % GRID_W).astype(jnp.float32)
    angles = jnp.concatenate([grid_row[:, None] * inverse, mesh_column[:, None] * inverse], axis=1)
    cosine = jnp.cos(angles)[:, None, :]
    sine_table = jnp.sin(angles)[:, None, :]
    shaped = projected.reshape(row_count, head_count, HEAD_SIZE)
    first_half = shaped[..., :half_dim]
    second = shaped[..., half_dim:]
    turned = jnp.concatenate(
        [first_half * cosine - second * sine_table, second * cosine + first_half * sine_table],
        axis=-1,
    )
    return turned.reshape(row_count, head_count * HEAD_SIZE)


def attend(
    queries, key_rows, value_rows, ctx_keys, ctx_values, sink_logit, q_begin, k_begin, seq_total
):
    row_count = queries.shape[0]
    key_count = key_rows.shape[0]
    ctx_count = ctx_keys.shape[0]
    kv_heads = key_rows.shape[1] // HEAD_SIZE
    head_count = queries.shape[1] // HEAD_SIZE
    group_size = head_count // kv_heads
    factor = 1.0 / math.sqrt(HEAD_SIZE)
    q_heads = queries.reshape(row_count, kv_heads, group_size, HEAD_SIZE)
    k_heads = key_rows.reshape(key_count, kv_heads, HEAD_SIZE)
    v_heads = value_rows.reshape(key_count, kv_heads, HEAD_SIZE)
    ck_heads = ctx_keys.reshape(ctx_count, kv_heads, HEAD_SIZE)
    cv_heads = ctx_values.reshape(ctx_count, kv_heads, HEAD_SIZE)
    near_scores = (
        jnp.einsum("qkgd,skd->kgqs", q_heads, k_heads, preferred_element_type=jnp.float32) * factor
    )
    q_pos = q_begin + jnp.arange(row_count, dtype=jnp.int32)
    k_pos = k_begin + jnp.arange(key_count, dtype=jnp.int32)
    in_window = (jnp.abs(q_pos[:, None] - k_pos[None, :]) <= WINDOW) & (
        (k_pos >= 0) & (k_pos < seq_total)
    )[None, :]
    near_scores = jnp.where(in_window, near_scores, MASK_VALUE)
    ctx_scores = (
        jnp.einsum("qkgd,skd->kgqs", q_heads, ck_heads, preferred_element_type=jnp.float32) * factor
    )
    sink_score = sink_logit.reshape(kv_heads, group_size)[:, :, None, None]
    peak_score = jnp.maximum(
        jnp.maximum(
            jnp.max(near_scores, axis=-1, keepdims=True),
            jnp.max(ctx_scores, axis=-1, keepdims=True),
        ),
        sink_score,
    )
    near_exp = jnp.exp(near_scores - peak_score)
    ctx_exp = jnp.exp(ctx_scores - peak_score)
    softmax_denominator = (
        jnp.sum(near_exp, axis=-1, keepdims=True)
        + jnp.sum(ctx_exp, axis=-1, keepdims=True)
        + jnp.exp(sink_score - peak_score)
    )
    near_weights = (near_exp / softmax_denominator).astype(jnp.bfloat16)
    ctx_weights = (ctx_exp / softmax_denominator).astype(jnp.bfloat16)
    result = jnp.einsum("kgqs,skd->qkgd", near_weights, v_heads, preferred_element_type=jnp.float32)
    result = result + jnp.einsum(
        "kgqs,skd->qkgd", ctx_weights, cv_heads, preferred_element_type=jnp.float32
    )
    return result.reshape(row_count, head_count * HEAD_SIZE)


def shards(
    latent,
    condition,
    ctx_condition,
    context,
    mod_shift,
    mod_scale,
    mod_gate,
    norm_gain,
    w_query,
    key_weight,
    value_weight,
    w_gate,
    w_out,
    sink_logit,
):
    latent_rows = lax.all_gather(latent, "tp", axis=0, tiled=True)
    sp_count = lax.axis_size("sp")
    sp_rank = lax.axis_index("sp")
    mod_rows = mod_shift.shape[0]
    cond_act = jax.nn.silu(condition).astype(jnp.bfloat16)
    ctx_act = jax.nn.silu(ctx_condition).astype(jnp.bfloat16)
    first_row = sp_rank * mod_rows
    lat_piece = lax.dynamic_slice_in_dim(cond_act, first_row, mod_rows, 0)
    ctx_piece = lax.dynamic_slice_in_dim(ctx_act, first_row, mod_rows, 0)
    both_conds = jnp.stack([lat_piece, ctx_piece])
    partial_value = jnp.concatenate(
        [
            jnp.dot(both_conds, mod_shift, preferred_element_type=jnp.float32),
            jnp.dot(both_conds, mod_scale, preferred_element_type=jnp.float32),
            jnp.dot(lat_piece[None, :], mod_gate, preferred_element_type=jnp.float32),
        ],
        axis=0,
    )
    summed = taken_together(partial_value, "sp")
    vectors = gather_directly(summed, "tp", 1)
    lat_shift = vectors[0]
    ctx_shift = vectors[1]
    lat_scale = vectors[2]
    ctx_scale = vectors[3]
    lat_gate = vectors[4]
    row_piece = modulate(latent_rows, norm_gain, lat_shift, lat_scale)
    ctx_hidden = modulate(context, norm_gain, ctx_shift, ctx_scale)
    kv_width = key_weight.shape[1]
    q_width = w_query.shape[1]
    ctx_pair = jnp.concatenate(
        [
            jnp.dot(ctx_hidden, key_weight, preferred_element_type=jnp.float32).astype(
                jnp.bfloat16
            ),
            jnp.dot(ctx_hidden, value_weight, preferred_element_type=jnp.float32).astype(
                jnp.bfloat16
            ),
        ],
        axis=1,
    )
    ctx_all = gather_directly(ctx_pair, "sp", 0)
    projected = jnp.concatenate(
        [
            jnp.dot(row_piece, w_query, preferred_element_type=jnp.float32),
            jnp.dot(row_piece, key_weight, preferred_element_type=jnp.float32),
            jnp.dot(row_piece, value_weight, preferred_element_type=jnp.float32),
            jnp.dot(row_piece, w_gate, preferred_element_type=jnp.float32),
        ],
        axis=1,
    )
    block_rows = projected.shape[0]
    q_begin = sp_rank * block_rows
    positions = q_begin + jnp.arange(block_rows, dtype=jnp.int32)
    queries = rotate(projected[:, :q_width], positions).astype(jnp.bfloat16)
    key_rows = rotate(projected[:, q_width : q_width + kv_width], positions).astype(jnp.bfloat16)
    value_rows = projected[:, q_width + kv_width : q_width + 2 * kv_width].astype(jnp.bfloat16)
    gate_proj = projected[:, q_width + 2 * kv_width :].astype(jnp.bfloat16)
    key_value = jnp.concatenate([key_rows, value_rows], axis=1)
    padded = with_halo(key_value, (("sp", 0),), WINDOW)
    attended = attend(
        queries,
        padded[:, :kv_width],
        padded[:, kv_width:],
        ctx_all[:, :kv_width],
        ctx_all[:, kv_width:],
        sink_logit,
        q_begin,
        q_begin - WINDOW,
        block_rows * sp_count,
    )
    mixed = (attended * jax.nn.silu(gate_proj.astype(jnp.float32))).astype(jnp.bfloat16)
    branch = lax.psum_scatter(
        jnp.dot(mixed, w_out, preferred_element_type=jnp.float32).astype(jnp.bfloat16),
        "tp",
        scatter_dimension=0,
        tiled=True,
    ).astype(jnp.float32)
    return (latent.astype(jnp.float32) + lat_gate * branch).astype(jnp.bfloat16)


def solution(mesh):
    return jax.shard_map(
        shards,
        mesh=mesh,
        in_specs=(
            P(("dp", "sp", "tp"), None),
            P("dp"),
            P(),
            P(("dp", "sp"), None),
            P("sp", "tp"),
            P("sp", "tp"),
            P("sp", "tp"),
            P(),
            P(None, "tp"),
            P(None, "tp"),
            P(None, "tp"),
            P(None, "tp"),
            P("tp", None),
            P("tp"),
        ),
        out_specs=P(("dp", "sp", "tp"), None),
        check_vma=False,
    )
```

```python
import math

import jax
import jax.numpy as jnp
from jax import lax
from jax.sharding import PartitionSpec as P

HEAD_SIZE = 64
WINDOW = 128
GRID_W = 64


NORM_EPS = 1e-06
MASK_VALUE = -1e30


def copy_for_each(shard, axis):
    copies = jnp.broadcast_to(shard, (lax.axis_size(axis), *shard.shape))
    return lax.all_to_all(copies, axis, split_axis=0, concat_axis=0, tiled=True)


def laid_out(tiles, dim):
    tiles = jnp.moveaxis(tiles, 0, dim)
    lengths = tiles.shape
    return tiles.reshape(*lengths[:dim], lengths[dim] * lengths[dim + 1], *lengths[dim + 2 :])


def gather_directly(shard, axis, dim):
    return laid_out(copy_for_each(shard, axis), dim)


def with_halo(block, sides, width):
    for axis, dim in sides:
        count = lax.axis_size(axis)
        forward = [(i, i + 1) for i in range(count - 1)]
        backward = [(target, source) for source, target in forward]
        low = lax.ppermute(
            lax.slice_in_dim(block, block.shape[dim] - width, None, axis=dim), axis, forward
        )
        high = lax.ppermute(lax.slice_in_dim(block, 0, width, axis=dim), axis, backward)
        block = jnp.concatenate([low, block, high], axis=dim)
    return block


def modulate(row_data, gain_vec, shift_vec, scale_vec):
    values = row_data.astype(jnp.float32)
    inverse = lax.rsqrt(jnp.mean(values * values, axis=-1, keepdims=True) + NORM_EPS)
    return (values * inverse * gain_vec * (1.0 + scale_vec) + shift_vec).astype(jnp.bfloat16)


def rotate(projected, positions):
    row_count = projected.shape[0]
    head_count = projected.shape[1] // HEAD_SIZE
    quarter = HEAD_SIZE // 4
    half_dim = HEAD_SIZE // 2
    inverse = jnp.exp(-math.log(10000.0) * jnp.arange(quarter, dtype=jnp.float32) / quarter)
    grid_row = (positions // GRID_W).astype(jnp.float32)
    mesh_column = (positions % GRID_W).astype(jnp.float32)
    angles = jnp.concatenate([grid_row[:, None] * inverse, mesh_column[:, None] * inverse], axis=1)
    cosine = jnp.cos(angles)[:, None, :]
    sine_table = jnp.sin(angles)[:, None, :]
    shaped = projected.reshape(row_count, head_count, HEAD_SIZE)
    first_half = shaped[..., :half_dim]
    second = shaped[..., half_dim:]
    turned = jnp.concatenate(
        [first_half * cosine - second * sine_table, second * cosine + first_half * sine_table],
        axis=-1,
    )
    return turned.reshape(row_count, head_count * HEAD_SIZE)


def attend(
    queries, key_rows, value_rows, ctx_keys, ctx_values, sink_logit, q_pos, k_begin, seq_total
):
    row_count = queries.shape[0]
    key_count = key_rows.shape[0]
    ctx_count = ctx_keys.shape[0]
    kv_heads = key_rows.shape[1] // HEAD_SIZE
    head_count = queries.shape[1] // HEAD_SIZE
    group_size = head_count // kv_heads
    factor = 1.0 / math.sqrt(HEAD_SIZE)
    q_heads = queries.reshape(row_count, kv_heads, group_size, HEAD_SIZE)
    k_heads = key_rows.reshape(key_count, kv_heads, HEAD_SIZE)
    v_heads = value_rows.reshape(key_count, kv_heads, HEAD_SIZE)
    ck_heads = ctx_keys.reshape(ctx_count, kv_heads, HEAD_SIZE)
    cv_heads = ctx_values.reshape(ctx_count, kv_heads, HEAD_SIZE)
    near_scores = (
        jnp.einsum("qkgd,skd->kgqs", q_heads, k_heads, preferred_element_type=jnp.float32) * factor
    )
    k_pos = k_begin + jnp.arange(key_count, dtype=jnp.int32)
    in_window = (jnp.abs(q_pos[:, None] - k_pos[None, :]) <= WINDOW) & (
        (k_pos >= 0) & (k_pos < seq_total)
    )[None, :]
    near_scores = jnp.where(in_window, near_scores, MASK_VALUE)
    ctx_scores = (
        jnp.einsum("qkgd,skd->kgqs", q_heads, ck_heads, preferred_element_type=jnp.float32) * factor
    )
    sink_score = sink_logit.reshape(kv_heads, group_size)[:, :, None, None]
    peak_score = jnp.maximum(
        jnp.maximum(
            jnp.max(near_scores, axis=-1, keepdims=True),
            jnp.max(ctx_scores, axis=-1, keepdims=True),
        ),
        sink_score,
    )
    near_exp = jnp.exp(near_scores - peak_score)
    ctx_exp = jnp.exp(ctx_scores - peak_score)
    softmax_denominator = (
        jnp.sum(near_exp, axis=-1, keepdims=True)
        + jnp.sum(ctx_exp, axis=-1, keepdims=True)
        + jnp.exp(sink_score - peak_score)
    )
    near_weights = (near_exp / softmax_denominator).astype(jnp.bfloat16)
    ctx_weights = (ctx_exp / softmax_denominator).astype(jnp.bfloat16)
    result = jnp.einsum("kgqs,skd->qkgd", near_weights, v_heads, preferred_element_type=jnp.float32)
    result = result + jnp.einsum(
        "kgqs,skd->qkgd", ctx_weights, cv_heads, preferred_element_type=jnp.float32
    )
    return result.reshape(row_count, head_count * HEAD_SIZE)


def shift(block, steps):
    count = lax.axis_size("tp")
    return lax.ppermute(block, "tp", [(i, (i + steps) % count) for i in range(count)])


def added(first, *others):
    total = first.astype(jnp.float32)
    for other in others:
        total = total + other.astype(jnp.float32)
    return total.astype(jnp.bfloat16)


def gather_rows(latent):
    half = latent.shape[1] // 2
    low2, high2 = shift(latent, 2), shift(latent, -2)
    low1, high1 = shift(latent, 1), shift(latent, -1)
    low3, high3 = shift(low2, 1), shift(high2, -1)
    far = jnp.concatenate([shift(low2[:, :half], 2), shift(high2[:, half:], -2)], axis=1)
    return [low3, low2, low1, latent, high1, high2, high3, far]


def reduce_rows(block):
    half = block(0).shape[1] // 2
    up3, down3 = shift(block(3), 1), shift(block(-3), -1)
    far = block(4)
    up4, down4 = shift(far[:, :half], 2), shift(far[:, half:], -2)
    up1, down1 = shift(block(1), 1), shift(block(-1), -1)
    gap = jnp.zeros_like(up4)
    two = added(block(2), up3, jnp.concatenate([up4, gap], axis=1))
    minus_two = added(block(-2), down3, jnp.concatenate([gap, down4], axis=1))
    up2, down2 = shift(two, 2), shift(minus_two, -2)
    total = block(0).astype(jnp.float32)
    for part in (up1, down1, up2, down2):
        total = total + part.astype(jnp.float32)
    return total


def body(
    latent,
    condition,
    ctx_condition,
    context,
    mod_shift,
    mod_scale,
    mod_gate,
    norm_gain,
    w_query,
    key_weight,
    value_weight,
    w_gate,
    w_out,
    sink_logit,
):
    tp_rank = lax.axis_index("tp")
    tp_count = lax.axis_size("tp")
    own_rows = latent.shape[0]
    pieces = gather_rows(latent)
    latent_rows = jnp.concatenate(pieces, axis=0)
    sp_count = lax.axis_size("sp")
    sp_rank = lax.axis_index("sp")
    mod_rows = mod_shift.shape[0]
    cond_act = jax.nn.silu(condition).astype(jnp.bfloat16)
    ctx_act = jax.nn.silu(ctx_condition).astype(jnp.bfloat16)
    first_row = sp_rank * mod_rows
    lat_piece = lax.dynamic_slice_in_dim(cond_act, first_row, mod_rows, 0)
    ctx_piece = lax.dynamic_slice_in_dim(ctx_act, first_row, mod_rows, 0)
    both_conds = jnp.stack([lat_piece, ctx_piece])
    partial_value = jnp.concatenate(
        [
            jnp.dot(both_conds, mod_shift, preferred_element_type=jnp.float32),
            jnp.dot(both_conds, mod_scale, preferred_element_type=jnp.float32),
            jnp.dot(lat_piece[None, :], mod_gate, preferred_element_type=jnp.float32),
        ],
        axis=0,
    )
    copies = copy_for_each(partial_value, "sp")
    summed = jnp.sum(copies, axis=0)
    vectors = copy_for_each(summed, "tp")
    vectors = laid_out(vectors, 1)
    lat_shift = vectors[0]
    ctx_shift = vectors[1]
    lat_scale = vectors[2]
    ctx_scale = vectors[3]
    lat_gate = vectors[4]
    row_piece = modulate(latent_rows, norm_gain, lat_shift, lat_scale)
    ctx_hidden = modulate(context, norm_gain, ctx_shift, ctx_scale)
    kv_width = key_weight.shape[1]
    q_width = w_query.shape[1]
    ctx_pair = jnp.concatenate(
        [
            jnp.dot(ctx_hidden, key_weight, preferred_element_type=jnp.float32).astype(
                jnp.bfloat16
            ),
            jnp.dot(ctx_hidden, value_weight, preferred_element_type=jnp.float32).astype(
                jnp.bfloat16
            ),
        ],
        axis=1,
    )
    ctx_all = gather_directly(ctx_pair, "sp", 0)
    projected = jnp.concatenate(
        [
            jnp.dot(row_piece, w_query, preferred_element_type=jnp.float32),
            jnp.dot(row_piece, key_weight, preferred_element_type=jnp.float32),
            jnp.dot(row_piece, value_weight, preferred_element_type=jnp.float32),
            jnp.dot(row_piece, w_gate, preferred_element_type=jnp.float32),
        ],
        axis=1,
    )
    block_rows = projected.shape[0]
    q_begin = sp_rank * block_rows
    local = jnp.arange(block_rows, dtype=jnp.int32)
    place = (tp_rank + tp_count - 3) * own_rows + local
    positions = q_begin + place % block_rows
    queries = rotate(projected[:, :q_width], positions).astype(jnp.bfloat16)
    key_rows = rotate(projected[:, q_width : q_width + kv_width], positions).astype(jnp.bfloat16)
    value_rows = projected[:, q_width + kv_width : q_width + 2 * kv_width].astype(jnp.bfloat16)
    gate_proj = projected[:, q_width + 2 * kv_width :].astype(jnp.bfloat16)
    key_value = jnp.concatenate([key_rows, value_rows], axis=1)
    key_value = lax.dynamic_slice_in_dim(
        jnp.concatenate([key_value, key_value], axis=0),
        (tp_count + 3 - tp_rank) % tp_count * own_rows,
        block_rows,
        0,
    )
    padded = with_halo(key_value, (("sp", 0),), WINDOW)
    attended = attend(
        queries,
        padded[:, :kv_width],
        padded[:, kv_width:],
        ctx_all[:, :kv_width],
        ctx_all[:, kv_width:],
        sink_logit,
        positions,
        q_begin - WINDOW,
        block_rows * sp_count,
    )
    mixed = (attended * jax.nn.silu(gate_proj.astype(jnp.float32))).astype(jnp.bfloat16)
    product = jnp.dot(mixed, w_out, preferred_element_type=jnp.float32).astype(jnp.bfloat16)
    branch = reduce_rows(lambda d: product[(d + 3) * own_rows : (d + 4) * own_rows])
    return (latent.astype(jnp.float32) + lat_gate * branch).astype(jnp.bfloat16)


def solution(mesh):
    return jax.shard_map(
        body,
        mesh=mesh,
        in_specs=(
            P(("dp", "sp", "tp"), None),
            P("dp"),
            P(),
            P(("dp", "sp"), None),
            P("sp", "tp"),
            P("sp", "tp"),
            P("sp", "tp"),
            P(),
            P(None, "tp"),
            P(None, "tp"),
            P(None, "tp"),
            P(None, "tp"),
            P("tp", None),
            P("tp"),
        ),
        out_specs=P(("dp", "sp", "tp"), None),
        check_vma=False,
    )
```

```python
import functools
import math

import jax
import jax.numpy as jnp
from jax import lax
from jax.experimental import pallas as pl
from jax.experimental.pallas import tpu as pltpu
from jax.sharding import PartitionSpec as P

HEAD_SIZE = 64
WINDOW = 128
GRID_W = 64
LANES = 128
NORM_EPS = 1e-06
MASK_VALUE = -1e30
VMEM = pl.BlockSpec(memory_space=pltpu.VMEM)
ANY = pl.BlockSpec(memory_space=pl.ANY)
SMEM = pl.BlockSpec(memory_space=pltpu.SMEM)


def rounded(values):
    return values.astype(jnp.bfloat16)


def contract(left, right, right_dim=0):
    return lax.dot_general(
        left, right, (((1,), (right_dim,)), ((), ())), preferred_element_type=jnp.float32
    )


def call(kernel, out_shape, *operands, specs=None, scratch=(), flops=10**9):
    return pl.pallas_call(
        kernel,
        out_shape=out_shape,
        in_specs=specs or [VMEM] * len(operands),
        out_specs=jax.tree.map(lambda _: VMEM, out_shape),
        scratch_shapes=scratch,
        compiler_params=pltpu.CompilerParams(vmem_limit_bytes=VMEM_GRANT),
        cost_estimate=pl.CostEstimate(flops=flops, bytes_accessed=10**6, transcendentals=0),
    )(*operands)


VMEM_GRANT = 30 * 2**20


def partial_kernel(acts, shift, scale, gate, out):
    sums = jnp.concatenate(
        [
            contract(acts[...], shift[...]),
            contract(acts[...], scale[...]),
            contract(acts[...], gate[...])[:1],
        ],
        axis=0,
    )
    for copy in range(out.shape[0]):
        out[copy] = sums


def total_kernel(parts, out):
    total = parts[0]
    for index in range(1, parts.shape[0]):
        total = total + parts[index]
    for copy in range(out.shape[0]):
        out[copy] = total


def modulated(pieces, vectors, gain, shift_row, scale_row, store):
    blocks, _, width = vectors.shape
    for read in pieces:
        square = None
        for block in range(blocks):
            values = read(block * width, width)
            part = sum(
                values[:, lane : lane + LANES] * values[:, lane : lane + LANES]
                for lane in range(0, width, LANES)
            )
            square = part if square is None else square + part
        mean = jnp.sum(square, axis=1, keepdims=True) / (blocks * width)
        inverse = lax.rsqrt(mean + NORM_EPS)
        for block in range(blocks):
            values = read(block * width, width)
            factor = gain[:, block * width : (block + 1) * width] * (
                1.0 + vectors[block, scale_row : scale_row + 1, :]
            )
            moved = values * inverse * factor + vectors[block, shift_row : shift_row + 1, :]
            store(read, block * width, rounded(moved))


def context_kernel(context, vectors, gain, kv_weight, out, hidden):
    def store(_, column, rows):
        hidden[:, column : column + rows.shape[1]] = rows

    modulated([lambda c, n: context[:, c : c + n].astype(jnp.float32)], vectors, gain, 1, 3, store)
    pair = rounded(contract(hidden[...], kv_weight[...], 1))
    for copy in range(out.shape[0]):
        out[copy] = pair


def turned(values, cosine, sine):
    lane = lax.broadcasted_iota(jnp.int32, values.shape, 1)
    half = HEAD_SIZE // 2
    other = jnp.where(
        lane % HEAD_SIZE < half, pltpu.roll(values, LANES - half, 1), pltpu.roll(values, half, 1)
    )
    return values * cosine + other * sine


def key_kernel(*refs, pieces, per_group):
    count = sum(len(piece) for piece in pieces)
    place, *blocks = refs[: 1 + count]
    vectors, gain, kv_weight, cosine, sine = refs[1 + count : 6 + count]
    hidden, key_value, first, last, ordered = refs[6 + count :]
    own = hidden.shape[0] // len(pieces)
    members = [[blocks.pop(0) for _ in piece] for piece in pieces]
    reads, places = [], {}
    for group in range(0, len(members), per_group):

        def read(column, columns, parts=members[group : group + per_group]):
            rows = []
            for part in parts:
                held = part[0].shape[1]
                ref, at = part[column // held], column % held
                rows.append(ref[:, at : at + columns].astype(jnp.float32))
            return jnp.concatenate(rows, axis=0) if len(rows) > 1 else rows[0]

        reads.append(read)
        places[read] = group * own

    def store(read, column, rows):
        begin = places[read]
        hidden[begin : begin + rows.shape[0], column : column + rows.shape[1]] = rows

    modulated(reads, vectors, gain, 0, 2, store)
    both = contract(hidden[...], kv_weight[...], 1)
    lane = lax.broadcasted_iota(jnp.int32, both.shape, 1)
    both = jnp.where(lane < HEAD_SIZE, turned(both, cosine[...], sine[...]), both)
    for index in range(len(pieces)):
        begin = pl.multiple_of(place[2 + index], 8)
        ordered[pl.ds(begin, own), :] = both[index * own : (index + 1) * own, :]
    key_value[...] = rounded(ordered[...])
    first[...] = rounded(ordered[:WINDOW, :])
    last[...] = rounded(ordered[ordered.shape[0] - WINDOW :, :])


def query_kernel(hidden, w_query, w_gate, cosine, sine, queries, gate, held, ready, *, own):
    fetch = pltpu.make_async_copy(w_gate, held, ready)
    fetch.start()
    rows, width = hidden.shape[0], w_query.shape[1]
    projected = contract(hidden[...], w_query[...])
    heads = width // HEAD_SIZE
    lane = lax.broadcasted_iota(jnp.int32, (rows, LANES), 1)
    for pair in range(width // LANES):
        tile = turned(projected[:, pair * LANES : (pair + 1) * LANES], cosine[...], sine[...])
        tile = tile * (1.0 / math.sqrt(HEAD_SIZE))
        for odd in range(2):
            head = 2 * pair + odd
            aligned = pltpu.roll(tile, HEAD_SIZE, 1) if odd else tile
            aligned = jnp.where(lane < HEAD_SIZE, aligned, 0.0)
            for block in range(rows // own):
                begin = (block * heads + head) * own
                queries[begin : begin + own, :] = aligned[block * own : (block + 1) * own, :]
    fetch.wait()
    gate[...] = rounded(contract(hidden[...], held[...])).astype(jnp.float32)


def attend_kernel(
    place,
    sink,
    queries,
    gate,
    low,
    middle,
    high,
    ctx,
    w_out,
    out,
    padded,
    mixed,
    held,
    ready,
    *,
    own,
    span,
):
    fetch = pltpu.make_async_copy(w_out, held, ready)
    fetch.start()
    rows = middle.shape[0]
    width = w_out.shape[0]
    heads = width // HEAD_SIZE
    padded[:WINDOW, :] = low[...].astype(jnp.float32)
    padded[WINDOW : WINDOW + rows, :] = middle[...].astype(jnp.float32)
    padded[WINDOW + rows : 2 * WINDOW + rows, :] = high[...].astype(jnp.float32)
    padded[2 * WINDOW + rows :, :] = jnp.zeros_like(padded[2 * WINDOW + rows :, :])
    row = lax.broadcasted_iota(jnp.int32, (own, span), 0)
    column = lax.broadcasted_iota(jnp.int32, (own, span), 1)
    in_reach = (column >= row) & (column <= row + 2 * WINDOW)
    lane = lax.broadcasted_iota(jnp.int32, (own, LANES), 1)
    sinks = jnp.concatenate([jnp.full((own, 1), sink[h], jnp.float32) for h in range(heads)], axis=0)
    blocks = rows // own
    for block in range(blocks):
        offset = pl.multiple_of(place[2 + block], 8)
        near = rounded(padded[pl.ds(offset, span), :])
        query = rounded(queries[block * heads * own : (block + 1) * heads * own, :])
        near_scores = contract(query, near, 1)
        ctx_scores = contract(query, ctx[...], 1)
        token = place[0] - WINDOW + offset + column
        seen = in_reach & (token >= 0) & (token < place[1])
        near_scores = jnp.where(
            seen[None], near_scores.reshape(heads, own, span), MASK_VALUE
        ).reshape(heads * own, span)
        peak = jnp.maximum(
            jnp.maximum(
                jnp.max(near_scores, axis=1, keepdims=True),
                jnp.max(ctx_scores, axis=1, keepdims=True),
            ),
            sinks,
        )
        near_exp = jnp.exp(near_scores - peak)
        ctx_exp = jnp.exp(ctx_scores - peak)
        denominator = (
            jnp.sum(near_exp, axis=1, keepdims=True)
            + jnp.sum(ctx_exp, axis=1, keepdims=True)
            + jnp.exp(sinks - peak)
        )
        inverse = 1.0 / denominator
        result = contract(rounded(near_exp * inverse), near) + contract(
            rounded(ctx_exp * inverse), ctx[...]
        )
        here = slice(block * own, (block + 1) * own)
        for pair in range(heads // 2):
            even = result[2 * pair * own : (2 * pair + 1) * own, :]
            odd = result[(2 * pair + 1) * own : (2 * pair + 2) * own, :]
            attended = jnp.where(lane < HEAD_SIZE, pltpu.roll(even, HEAD_SIZE, 1), odd)
            tile = gate[here, pair * LANES : (pair + 1) * LANES]
            mixed[here, pair * LANES : (pair + 1) * LANES] = attended * (
                tile / (1.0 + jnp.exp(-tile))
            )
    fetch.wait()
    final = rounded(mixed[...])
    step = 512
    for begin in range(0, w_out.shape[1], step):
        out[:, begin : begin + step] = rounded(contract(final, held[:, begin : begin + step]))


def copy_for_each(copies, axis):
    return lax.all_to_all(copies, axis, split_axis=0, concat_axis=0, tiled=True)


def shift(block, axis, steps, wrap=True):
    count = lax.axis_size(axis)
    pairs = [(i, (i + steps) % count) for i in range(count) if wrap or 0 <= i + steps < count]
    return lax.ppermute(block, axis, pairs)


def added(first, *others):
    total = first.astype(jnp.float32)
    for other in others:
        total = total + other.astype(jnp.float32)
    return rounded(total)


def gather_rows(latent):
    half = latent.shape[1] // 2
    low2, high2 = shift(latent, "tp", 2), shift(latent, "tp", -2)
    low1, high1 = shift(latent, "tp", 1), shift(latent, "tp", -1)
    far = (shift(low2[:, :half], "tp", 2), shift(high2[:, half:], "tp", -2))
    low3, high3 = shift(low2, "tp", 1), shift(high2, "tp", -1)
    return [(low3,), (low2,), (low1,), (latent,), (high1,), (high2,), (high3,), far]


def reduce_rows(block):
    half = block(0).shape[1] // 2
    far = block(4)
    up4, down4 = shift(far[:, :half], "tp", 2), shift(far[:, half:], "tp", -2)
    up3, down3 = shift(block(3), "tp", 1), shift(block(-3), "tp", -1)
    up1, down1 = shift(block(1), "tp", 1), shift(block(-1), "tp", -1)
    gap = jnp.zeros_like(up4)
    two = added(block(2), up3, jnp.concatenate([up4, gap], axis=1))
    minus_two = added(block(-2), down3, jnp.concatenate([gap, down4], axis=1))
    up2, down2 = shift(two, "tp", 2), shift(minus_two, "tp", -2)
    total = block(0).astype(jnp.float32)
    for part in (up1, down1, up2, down2):
        total = total + part.astype(jnp.float32)
    return total


def angle_tables(positions):
    quarter = HEAD_SIZE // 4
    lane = jnp.arange(LANES, dtype=jnp.int32)
    entry = lane % (2 * quarter)
    exponent = (entry % quarter).astype(jnp.float32)
    inverse = jnp.exp(-math.log(10000.0) * exponent / quarter)
    grid_row = (positions // GRID_W).astype(jnp.float32)[:, None]
    grid_column = (positions % GRID_W).astype(jnp.float32)[:, None]
    angles = jnp.where(entry < quarter, grid_row, grid_column) * inverse
    sign = jnp.where(lane % HEAD_SIZE < HEAD_SIZE // 2, -1.0, 1.0)
    return jnp.cos(angles), jnp.sin(angles) * sign


def body(
    latent,
    condition,
    ctx_condition,
    context,
    mod_shift,
    mod_scale,
    mod_gate,
    norm_gain,
    w_query,
    key_weight,
    value_weight,
    w_gate,
    w_out,
    sink_logit,
):
    f32, bf16 = jnp.float32, jnp.bfloat16
    shape = jax.ShapeDtypeStruct
    sp_count, sp_rank = lax.axis_size("sp"), lax.axis_index("sp")
    tp_count, tp_rank = lax.axis_size("tp"), lax.axis_index("tp")
    own, width = latent.shape
    rows = own * tp_count
    mod_rows, columns = mod_shift.shape
    behind = (tp_count - 1) // 2

    conditions = jnp.stack(
        [
            lax.dynamic_slice_in_dim(vector, sp_rank * mod_rows, mod_rows, 0)
            for vector in (condition, ctx_condition)
        ]
    )
    acts = rounded(jax.nn.silu(conditions))
    parts = call(
        partial_kernel, shape((sp_count, 5, columns), f32), acts, mod_shift, mod_scale, mod_gate
    )
    pieces = gather_rows(latent)
    parts = copy_for_each(parts, "sp")
    totals = call(total_kernel, shape((tp_count, 5, columns), f32), parts)
    vectors = copy_for_each(totals, "tp")

    gain = norm_gain[None, :]
    kv_weight = jnp.concatenate([key_weight.T, value_weight.T], axis=0)
    offsets = (
        (tp_rank + tp_count - behind + jnp.arange(tp_count, dtype=jnp.int32)) % tp_count * own
    )
    begin = sp_rank * rows
    positions = begin + (offsets[:, None] + jnp.arange(own, dtype=jnp.int32)).reshape(rows)
    cosine, sine = angle_tables(positions)
    place = jnp.concatenate([jnp.stack([begin, rows * sp_count]).astype(jnp.int32), offsets])

    ctx_rows = context.shape[0]
    ctx_pair = call(
        context_kernel,
        shape((sp_count, ctx_rows, LANES), bf16),
        context,
        vectors,
        gain,
        kv_weight,
        scratch=[pltpu.VMEM((ctx_rows, width), bf16)],
    )
    ctx_all = copy_for_each(ctx_pair, "sp").reshape(sp_count * ctx_rows, LANES)

    blocks = [block for piece in pieces for block in piece]
    hidden, key_value, first, last = call(
        functools.partial(key_kernel, pieces=[[0] * len(p) for p in pieces], per_group=2),
        [
            shape((rows, width), bf16),
            shape((rows, LANES), bf16),
            shape((WINDOW, LANES), bf16),
            shape((WINDOW, LANES), bf16),
        ],
        place,
        *blocks,
        vectors,
        gain,
        kv_weight,
        cosine,
        sine,
        specs=[SMEM] + [VMEM] * (len(blocks) + 5),
        scratch=[pltpu.VMEM((rows, LANES), f32)],
    )
    low = shift(last, "sp", 1, wrap=False)
    high = shift(first, "sp", -1, wrap=False)
    heads = w_query.shape[1] // HEAD_SIZE
    queries, gate = call(
        functools.partial(query_kernel, own=own),
        [shape((rows * heads, LANES), f32), shape((rows, w_gate.shape[1]), f32)],
        hidden,
        w_query,
        w_gate,
        cosine,
        sine,
        specs=[VMEM, VMEM, ANY, VMEM, VMEM],
        scratch=[pltpu.VMEM(w_gate.shape, bf16), pltpu.SemaphoreType.DMA],
        flops=2 * 10**9,
    )
    span = 3 * LANES
    product = call(
        functools.partial(attend_kernel, own=own, span=span),
        shape((rows, width), bf16),
        place,
        sink_logit,
        queries,
        gate,
        low,
        key_value,
        high,
        ctx_all,
        w_out,
        specs=[SMEM, SMEM] + [VMEM] * 6 + [ANY],
        scratch=[
            pltpu.VMEM((rows - own + span, LANES), f32),
            pltpu.VMEM((rows, w_out.shape[0]), f32),
            pltpu.VMEM(w_out.shape, bf16),
            pltpu.SemaphoreType.DMA,
        ],
        flops=3 * 10**9,
    )
    branch = reduce_rows(lambda d: product[(d + behind) * own : (d + behind + 1) * own])
    lat_gate = vectors[:, 4, :].reshape(width)
    return rounded(latent.astype(f32) + lat_gate * branch)


def solution(mesh):
    return jax.shard_map(
        body,
        mesh=mesh,
        in_specs=(
            P(("dp", "sp", "tp"), None),
            P("dp"),
            P(),
            P(("dp", "sp"), None),
            P("sp", "tp"),
            P("sp", "tp"),
            P("sp", "tp"),
            P(),
            P(None, "tp"),
            P(None, "tp"),
            P(None, "tp"),
            P(None, "tp"),
            P("tp", None),
            P("tp"),
        ),
        out_specs=P(("dp", "sp", "tp"), None),
        check_vma=False,
    )
```

```python
import functools
import math

import jax
import jax.numpy as jnp
from jax import lax
from jax.experimental import pallas as pl
from jax.experimental.pallas import tpu as pltpu
from jax.sharding import PartitionSpec as P

HEAD_SIZE = 64
WINDOW = 128
GRID_W = 64
LANES = 128
NORM_EPS = 1e-06
MASK_VALUE = -1e30
VMEM = pl.BlockSpec(memory_space=pltpu.VMEM)
HBM = pl.BlockSpec(memory_space=pltpu.HBM)
SMEM = pl.BlockSpec(memory_space=pltpu.SMEM)


def rounded(values):
    return values.astype(jnp.bfloat16)


def contract(left, right, right_dim=0):
    return lax.dot_general(
        left, right, (((1,), (right_dim,)), ((), ())), preferred_element_type=jnp.float32
    )


def call(kernel, out_shape, *operands, specs=None, scratch=(), flops=10**9, grant=30):
    return pl.pallas_call(
        kernel,
        out_shape=out_shape,
        in_specs=specs or [VMEM] * len(operands),
        out_specs=jax.tree.map(lambda _: VMEM, out_shape),
        scratch_shapes=scratch,
        compiler_params=pltpu.CompilerParams(vmem_limit_bytes=grant * 2**20),
        cost_estimate=pl.CostEstimate(flops=flops, bytes_accessed=10**6, transcendentals=0),
    )(*operands)


def partial_kernel(rank, conditions, shift, scale, gate, out, held, ready):
    fetches = []
    for index, weight in enumerate((shift, scale, gate)):
        fetches.append(pltpu.make_async_copy(weight, held.at[index], ready.at[index]))
        fetches[-1].start()
    mine = pl.ds(rank[0], 1)
    values = jnp.concatenate([conditions[0, mine, :], conditions[1, mine, :]], axis=0)
    acts = rounded(values / (1.0 + jnp.exp(-values)))
    sums = []
    for index, fetch in enumerate(fetches):
        fetch.wait()
        sums.append(contract(acts, held[index]))
    sums = jnp.concatenate([sums[0], sums[1], sums[2][:1]], axis=0)
    for copy in range(out.shape[0]):
        out[copy] = sums


def total_kernel(parts, out):
    total = parts[0]
    for index in range(1, parts.shape[0]):
        total = total + parts[index]
    for copy in range(out.shape[0]):
        out[copy] = total


def modulated(pieces, vectors, gain, shift_row, scale_row, store):
    blocks, _, width = vectors.shape
    for read in pieces:
        square = None
        for block in range(blocks):
            values = read(block * width, width)
            part = sum(
                values[:, lane : lane + LANES] * values[:, lane : lane + LANES]
                for lane in range(0, width, LANES)
            )
            square = part if square is None else square + part
        mean = jnp.sum(square, axis=1, keepdims=True) / (blocks * width)
        inverse = lax.rsqrt(mean + NORM_EPS)
        for block in range(blocks):
            values = read(block * width, width)
            factor = gain[:, block * width : (block + 1) * width] * (
                1.0 + vectors[block, scale_row : scale_row + 1, :]
            )
            moved = values * inverse * factor + vectors[block, shift_row : shift_row + 1, :]
            store(read, block * width, rounded(moved))


def context_kernel(context, vectors, gain, kv_weight, out, hidden):
    def store(_, column, rows):
        hidden[:, column : column + rows.shape[1]] = rows

    modulated([lambda c, n: context[:, c : c + n].astype(jnp.float32)], vectors, gain, 1, 3, store)
    pair = rounded(contract(hidden[...], kv_weight[...], 1))
    for copy in range(out.shape[0]):
        out[copy] = pair


def turned(values, cosine, sine):
    lane = lax.broadcasted_iota(jnp.int32, values.shape, 1)
    half = HEAD_SIZE // 2
    other = jnp.where(
        lane % HEAD_SIZE < half, pltpu.roll(values, LANES - half, 1), pltpu.roll(values, half, 1)
    )
    return values * cosine + other * sine


def key_kernel(*refs, pieces, per_group):
    count = sum(len(piece) for piece in pieces)
    place, *blocks = refs[: 1 + count]
    vectors, gain, kv_weight, cosine, sine = refs[1 + count : 6 + count]
    hidden, key_value, first, last, ordered = refs[6 + count :]
    own = hidden.shape[0] // len(pieces)
    members = [[blocks.pop(0) for _ in piece] for piece in pieces]
    reads, places = [], {}
    for group in range(0, len(members), per_group):

        def read(column, columns, parts=members[group : group + per_group]):
            rows = []
            for part in parts:
                held = part[0].shape[1]
                ref, at = part[column // held], column % held
                rows.append(ref[:, at : at + columns].astype(jnp.float32))
            return jnp.concatenate(rows, axis=0) if len(rows) > 1 else rows[0]

        reads.append(read)
        places[read] = group * own

    def store(read, column, rows):
        begin = places[read]
        hidden[begin : begin + rows.shape[0], column : column + rows.shape[1]] = rows

    modulated(reads, vectors, gain, 0, 2, store)
    both = contract(hidden[...], kv_weight[...], 1)
    lane = lax.broadcasted_iota(jnp.int32, both.shape, 1)
    both = jnp.where(lane < HEAD_SIZE, turned(both, cosine[...], sine[...]), both)
    for index in range(len(pieces)):
        begin = pl.multiple_of(place[2 + index], 8)
        ordered[pl.ds(begin, own), :] = both[index * own : (index + 1) * own, :]
    key_value[...] = rounded(ordered[...])
    first[...] = rounded(ordered[:WINDOW, :])
    last[...] = rounded(ordered[ordered.shape[0] - WINDOW :, :])


def query_kernel(hidden, w_query, w_gate, cosine, sine, queries, gate, held, ready, *, own):
    fetch = pltpu.make_async_copy(w_gate, held, ready)
    fetch.start()
    rows, width = hidden.shape[0], w_query.shape[1]
    projected = contract(hidden[...], w_query[...])
    heads = width // HEAD_SIZE
    lane = lax.broadcasted_iota(jnp.int32, (rows, LANES), 1)
    for pair in range(width // LANES):
        tile = turned(projected[:, pair * LANES : (pair + 1) * LANES], cosine[...], sine[...])
        tile = tile * (1.0 / math.sqrt(HEAD_SIZE))
        for odd in range(2):
            head = 2 * pair + odd
            aligned = pltpu.roll(tile, HEAD_SIZE, 1) if odd else tile
            aligned = jnp.where(lane < HEAD_SIZE, aligned, 0.0)
            for block in range(rows // own):
                begin = (block * heads + head) * own
                queries[begin : begin + own, :] = aligned[block * own : (block + 1) * own, :]
    fetch.wait()
    gate[...] = rounded(contract(hidden[...], held[...])).astype(jnp.float32)


def attend_kernel(
    place,
    sink,
    queries,
    gate,
    low,
    middle,
    high,
    ctx,
    w_out,
    out,
    padded,
    mixed,
    held,
    ready,
    *,
    own,
    span,
):
    fetch = pltpu.make_async_copy(w_out, held, ready)
    fetch.start()
    rows = middle.shape[0]
    width = w_out.shape[0]
    heads = width // HEAD_SIZE
    padded[:WINDOW, :] = low[...].astype(jnp.float32)
    padded[WINDOW : WINDOW + rows, :] = middle[...].astype(jnp.float32)
    padded[WINDOW + rows : 2 * WINDOW + rows, :] = high[...].astype(jnp.float32)
    padded[2 * WINDOW + rows :, :] = jnp.zeros_like(padded[2 * WINDOW + rows :, :])
    row = lax.broadcasted_iota(jnp.int32, (own, span), 0)
    column = lax.broadcasted_iota(jnp.int32, (own, span), 1)
    in_reach = (column >= row) & (column <= row + 2 * WINDOW)
    lane = lax.broadcasted_iota(jnp.int32, (own, LANES), 1)
    sinks = jnp.concatenate([jnp.full((own, 1), sink[h], jnp.float32) for h in range(heads)], axis=0)
    blocks = rows // own
    for block in range(blocks):
        offset = pl.multiple_of(place[2 + block], 8)
        near = rounded(padded[pl.ds(offset, span), :])
        query = rounded(queries[block * heads * own : (block + 1) * heads * own, :])
        near_scores = contract(query, near, 1)
        ctx_scores = contract(query, ctx[...], 1)
        token = place[0] - WINDOW + offset + column
        seen = in_reach & (token >= 0) & (token < place[1])
        near_scores = jnp.where(
            seen[None], near_scores.reshape(heads, own, span), MASK_VALUE
        ).reshape(heads * own, span)
        peak = jnp.maximum(
            jnp.maximum(
                jnp.max(near_scores, axis=1, keepdims=True),
                jnp.max(ctx_scores, axis=1, keepdims=True),
            ),
            sinks,
        )
        near_exp = jnp.exp(near_scores - peak)
        ctx_exp = jnp.exp(ctx_scores - peak)
        denominator = (
            jnp.sum(near_exp, axis=1, keepdims=True)
            + jnp.sum(ctx_exp, axis=1, keepdims=True)
            + jnp.exp(sinks - peak)
        )
        inverse = 1.0 / denominator
        result = contract(rounded(near_exp * inverse), near) + contract(
            rounded(ctx_exp * inverse), ctx[...]
        )
        here = slice(block * own, (block + 1) * own)
        for pair in range(heads // 2):
            even = result[2 * pair * own : (2 * pair + 1) * own, :]
            odd = result[(2 * pair + 1) * own : (2 * pair + 2) * own, :]
            attended = jnp.where(lane < HEAD_SIZE, pltpu.roll(even, HEAD_SIZE, 1), odd)
            tile = gate[here, pair * LANES : (pair + 1) * LANES]
            mixed[here, pair * LANES : (pair + 1) * LANES] = attended * (
                tile / (1.0 + jnp.exp(-tile))
            )
    fetch.wait()
    final = rounded(mixed[...])
    step = 512
    for begin in range(0, w_out.shape[1], step):
        out[:, begin : begin + step] = rounded(contract(final, held[:, begin : begin + step]))


def copy_for_each(copies, axis):
    return lax.all_to_all(copies, axis, split_axis=0, concat_axis=0, tiled=True)


def shift(block, axis, steps, wrap=True):
    count = lax.axis_size(axis)
    pairs = [(i, (i + steps) % count) for i in range(count) if wrap or 0 <= i + steps < count]
    return lax.ppermute(block, axis, pairs)


def added(first, *others):
    total = first.astype(jnp.float32)
    for other in others:
        total = total + other.astype(jnp.float32)
    return rounded(total)


def shift_by_parity(block, steps):
    tp_count, dp_count = lax.axis_size("tp"), lax.axis_size("dp")
    pairs = []
    for i in range(tp_count):
        for j in range(dp_count):
            target = (i + (steps if j % 2 == 0 else -steps)) % tp_count
            pairs.append((i * dp_count + j, target * dp_count + j))
    return lax.ppermute(block, ("tp", "dp"), pairs)


def gather_rows(latent, even):
    low2, high2 = shift(latent, "tp", 2), shift(latent, "tp", -2)
    low1, high1 = shift(latent, "tp", 1), shift(latent, "tp", -1)
    far = shift_by_parity(jnp.where(even, low2, high2), 2)
    low3, high3 = shift(low2, "tp", 1), shift(high2, "tp", -1)
    return [(low3,), (low2,), (low1,), (latent,), (high1,), (high2,), (high3,), (far,)]


def reduce_rows(block, even):
    far = shift_by_parity(block(4), 2)
    up3, down3 = shift(block(3), "tp", 1), shift(block(-3), "tp", -1)
    nothing = jnp.zeros_like(far)
    two = added(block(2), up3, jnp.where(even, far, nothing))
    minus_two = added(block(-2), down3, jnp.where(even, nothing, far))
    up2, down2 = shift(two, "tp", 2), shift(minus_two, "tp", -2)
    up1, down1 = shift(block(1), "tp", 1), shift(block(-1), "tp", -1)
    total = block(0).astype(jnp.float32)
    for part in (up1, down1, up2, down2):
        total = total + part.astype(jnp.float32)
    return total


def angle_tables(positions):
    quarter = HEAD_SIZE // 4
    lane = jnp.arange(LANES, dtype=jnp.int32)
    entry = lane % (2 * quarter)
    exponent = (entry % quarter).astype(jnp.float32)
    inverse = jnp.exp(-math.log(10000.0) * exponent / quarter)
    grid_row = (positions // GRID_W).astype(jnp.float32)[:, None]
    grid_column = (positions % GRID_W).astype(jnp.float32)[:, None]
    angles = jnp.where(entry < quarter, grid_row, grid_column) * inverse
    sign = jnp.where(lane % HEAD_SIZE < HEAD_SIZE // 2, -1.0, 1.0)
    return jnp.cos(angles), jnp.sin(angles) * sign


def body(
    latent,
    condition,
    ctx_condition,
    context,
    mod_shift,
    mod_scale,
    mod_gate,
    norm_gain,
    w_query,
    key_weight,
    value_weight,
    w_gate,
    w_out,
    sink_logit,
):
    f32, bf16 = jnp.float32, jnp.bfloat16
    shape = jax.ShapeDtypeStruct
    sp_count, sp_rank = lax.axis_size("sp"), lax.axis_index("sp")
    tp_count, tp_rank = lax.axis_size("tp"), lax.axis_index("tp")
    own, width = latent.shape
    rows = own * tp_count
    mod_rows, columns = mod_shift.shape
    behind = (tp_count - 1) // 2

    conditions = jnp.stack([condition, ctx_condition]).reshape(2, sp_count, mod_rows)
    parts = call(
        partial_kernel,
        shape((sp_count, 5, columns), f32),
        sp_rank.astype(jnp.int32)[None],
        conditions,
        mod_shift,
        mod_scale,
        mod_gate,
        specs=[SMEM, VMEM, HBM, HBM, HBM],
        scratch=[pltpu.VMEM((3, mod_rows, columns), bf16), pltpu.SemaphoreType.DMA((3,))],
        grant=63,
    )
    even = lax.axis_index("dp") % 2 == 0
    pieces = gather_rows(latent, even)
    parts = copy_for_each(parts, "sp")
    totals = call(total_kernel, shape((tp_count, 5, columns), f32), parts)
    vectors = copy_for_each(totals, "tp")

    gain = norm_gain[None, :]
    kv_weight = jnp.concatenate([key_weight.T, value_weight.T], axis=0)
    offsets = (
        (tp_rank + tp_count - behind + jnp.arange(tp_count, dtype=jnp.int32)) % tp_count * own
    )
    begin = sp_rank * rows
    positions = begin + (offsets[:, None] + jnp.arange(own, dtype=jnp.int32)).reshape(rows)
    cosine, sine = angle_tables(positions)
    place = jnp.concatenate([jnp.stack([begin, rows * sp_count]).astype(jnp.int32), offsets])

    ctx_rows = context.shape[0]
    ctx_pair = call(
        context_kernel,
        shape((sp_count, ctx_rows, LANES), bf16),
        context,
        vectors,
        gain,
        kv_weight,
        scratch=[pltpu.VMEM((ctx_rows, width), bf16)],
    )
    ctx_all = copy_for_each(ctx_pair, "sp").reshape(sp_count * ctx_rows, LANES)

    blocks = [block for piece in pieces for block in piece]
    hidden, key_value, first, last = call(
        functools.partial(key_kernel, pieces=[[0] * len(p) for p in pieces], per_group=2),
        [
            shape((rows, width), bf16),
            shape((rows, LANES), bf16),
            shape((WINDOW, LANES), bf16),
            shape((WINDOW, LANES), bf16),
        ],
        place,
        *blocks,
        vectors,
        gain,
        kv_weight,
        cosine,
        sine,
        specs=[SMEM] + [VMEM] * (len(blocks) + 5),
        scratch=[pltpu.VMEM((rows, LANES), f32)],
    )
    low = shift(last, "sp", 1, wrap=False)
    high = shift(first, "sp", -1, wrap=False)
    heads = w_query.shape[1] // HEAD_SIZE
    queries, gate = call(
        functools.partial(query_kernel, own=own),
        [shape((rows * heads, LANES), f32), shape((rows, w_gate.shape[1]), f32)],
        hidden,
        w_query,
        w_gate,
        cosine,
        sine,
        specs=[VMEM, VMEM, HBM, VMEM, VMEM],
        scratch=[pltpu.VMEM(w_gate.shape, bf16), pltpu.SemaphoreType.DMA],
        flops=2 * 10**9,
        grant=48,
    )
    span = 3 * LANES
    product = call(
        functools.partial(attend_kernel, own=own, span=span),
        shape((rows, width), bf16),
        place,
        sink_logit,
        queries,
        gate,
        low,
        key_value,
        high,
        ctx_all,
        w_out,
        specs=[SMEM, SMEM] + [VMEM] * 6 + [HBM],
        scratch=[
            pltpu.VMEM((rows - own + span, LANES), f32),
            pltpu.VMEM((rows, w_out.shape[0]), f32),
            pltpu.VMEM(w_out.shape, bf16),
            pltpu.SemaphoreType.DMA,
        ],
        flops=3 * 10**9,
        grant=50,
    )
    branch = reduce_rows(lambda d: product[(d + behind) * own : (d + behind + 1) * own], even)
    lat_gate = vectors[:, 4, :].reshape(width)
    return rounded(latent.astype(f32) + lat_gate * branch)


def solution(mesh):
    return jax.shard_map(
        body,
        mesh=mesh,
        in_specs=(
            P(("dp", "sp", "tp"), None),
            P("dp"),
            P(),
            P(("dp", "sp"), None),
            P("sp", "tp"),
            P("sp", "tp"),
            P("sp", "tp"),
            P(),
            P(None, "tp"),
            P(None, "tp"),
            P(None, "tp"),
            P(None, "tp"),
            P("tp", None),
            P("tp"),
        ),
        out_specs=P(("dp", "sp", "tp"), None),
        check_vma=False,
    )
```

```python
import functools
import math

import jax
import jax.numpy as jnp
from jax import lax
from jax.experimental import pallas as pl
from jax.experimental.pallas import tpu as pltpu
from jax.sharding import PartitionSpec as P

HEAD_SIZE = 64
WINDOW = 128
GRID_W = 64
LANES = 128
NORM_EPS = 1e-06
MASK_VALUE = -1e30
VMEM = pl.BlockSpec(memory_space=pltpu.VMEM)
HBM = pl.BlockSpec(memory_space=pltpu.HBM)
SMEM = pl.BlockSpec(memory_space=pltpu.SMEM)


def rounded(values):
    return values.astype(jnp.bfloat16)


def contract(left, right, right_dim=0):
    return lax.dot_general(
        left, right, (((1,), (right_dim,)), ((), ())), preferred_element_type=jnp.float32
    )


def call(kernel, out_shape, *operands, specs=None, scratch=(), flops=10**9, grant=30):
    return pl.pallas_call(
        kernel,
        out_shape=out_shape,
        in_specs=specs or [VMEM] * len(operands),
        out_specs=jax.tree.map(lambda _: VMEM, out_shape),
        scratch_shapes=scratch,
        compiler_params=pltpu.CompilerParams(vmem_limit_bytes=grant * 2**20),
        cost_estimate=pl.CostEstimate(flops=flops, bytes_accessed=10**6, transcendentals=0),
    )(*operands)


def partial_kernel(rank, condition, ctx_condition, shift, scale, gate, out, held, ready):
    fetches = []
    for index, weight in enumerate((shift, scale, gate)):
        fetches.append(pltpu.make_async_copy(weight, held.at[index], ready.at[index]))
        fetches[-1].start()
    mine = pl.ds(pl.multiple_of(rank[0] * held.shape[1], held.shape[1]), held.shape[1])
    values = jnp.stack([condition[mine], ctx_condition[mine]])
    acts = rounded(values / (1.0 + jnp.exp(-values)))
    sums = []
    for index, fetch in enumerate(fetches):
        fetch.wait()
        sums.append(contract(acts, held[index]))
    sums = jnp.concatenate([sums[0], sums[1], sums[2][:1]], axis=0)
    for copy in range(out.shape[0]):
        out[copy] = sums


def total_kernel(parts, out):
    total = parts[0]
    for index in range(1, parts.shape[0]):
        total = total + parts[index]
    for copy in range(out.shape[0]):
        out[copy] = total


def modulated(pieces, vectors, gain, shift_row, scale_row, store):
    blocks, _, width = vectors.shape
    for read in pieces:
        square = None
        for block in range(blocks):
            values = read(block * width, width)
            part = sum(
                values[:, lane : lane + LANES] * values[:, lane : lane + LANES]
                for lane in range(0, width, LANES)
            )
            square = part if square is None else square + part
        mean = jnp.sum(square, axis=1, keepdims=True) / (blocks * width)
        inverse = lax.rsqrt(mean + NORM_EPS)
        for block in range(blocks):
            values = read(block * width, width)
            factor = gain[:, block * width : (block + 1) * width] * (
                1.0 + vectors[block, scale_row : scale_row + 1, :]
            )
            moved = values * inverse * factor + vectors[block, shift_row : shift_row + 1, :]
            store(read, block * width, rounded(moved))


def context_kernel(context, vectors, gain, kv_weight, out, hidden):
    def store(_, column, rows):
        hidden[:, column : column + rows.shape[1]] = rows

    modulated([lambda c, n: context[:, c : c + n].astype(jnp.float32)], vectors, gain, 1, 3, store)
    pair = rounded(contract(hidden[...], kv_weight[...], 1))
    for copy in range(out.shape[0]):
        out[copy] = pair


def turned(values, cosine, sine):
    lane = lax.broadcasted_iota(jnp.int32, values.shape, 1)
    half = HEAD_SIZE // 2
    other = jnp.where(
        lane % HEAD_SIZE < half, pltpu.roll(values, LANES - half, 1), pltpu.roll(values, half, 1)
    )
    return values * cosine + other * sine


def key_kernel(*refs, pieces, per_group):
    count = sum(len(piece) for piece in pieces)
    place, *blocks = refs[: 1 + count]
    vectors, gain, kv_weight, cosine, sine = refs[1 + count : 6 + count]
    hidden, key_value, first, last, ordered = refs[6 + count :]
    own = hidden.shape[0] // len(pieces)
    members = [[blocks.pop(0) for _ in piece] for piece in pieces]
    reads, places = [], {}
    for group in range(0, len(members), per_group):

        def read(column, columns, parts=members[group : group + per_group]):
            rows = []
            for part in parts:
                held = part[0].shape[1]
                ref, at = part[column // held], column % held
                rows.append(ref[:, at : at + columns].astype(jnp.float32))
            return jnp.concatenate(rows, axis=0) if len(rows) > 1 else rows[0]

        reads.append(read)
        places[read] = group * own

    def store(read, column, rows):
        begin = places[read]
        hidden[begin : begin + rows.shape[0], column : column + rows.shape[1]] = rows

    modulated(reads, vectors, gain, 0, 2, store)
    both = contract(hidden[...], kv_weight[...], 1)
    lane = lax.broadcasted_iota(jnp.int32, both.shape, 1)
    both = jnp.where(lane < HEAD_SIZE, turned(both, cosine[...], sine[...]), both)
    for index in range(len(pieces)):
        begin = pl.multiple_of(place[2 + index], 8)
        ordered[pl.ds(begin, own), :] = both[index * own : (index + 1) * own, :]
    key_value[...] = rounded(ordered[...])
    first[...] = rounded(ordered[:WINDOW, :])
    last[...] = rounded(ordered[ordered.shape[0] - WINDOW :, :])


def query_kernel(hidden, w_query, w_gate, cosine, sine, queries, gate, held, ready, *, own):
    fetch = pltpu.make_async_copy(w_gate, held, ready)
    fetch.start()
    rows, width = hidden.shape[0], w_query.shape[1]
    projected = contract(hidden[...], w_query[...])
    heads = width // HEAD_SIZE
    lane = lax.broadcasted_iota(jnp.int32, (rows, LANES), 1)
    for pair in range(width // LANES):
        tile = turned(projected[:, pair * LANES : (pair + 1) * LANES], cosine[...], sine[...])
        tile = tile * (1.0 / math.sqrt(HEAD_SIZE))
        for odd in range(2):
            head = 2 * pair + odd
            aligned = pltpu.roll(tile, HEAD_SIZE, 1) if odd else tile
            aligned = jnp.where(lane < HEAD_SIZE, aligned, 0.0)
            for block in range(rows // own):
                begin = (block * heads + head) * own
                queries[begin : begin + own, :] = aligned[block * own : (block + 1) * own, :]
    fetch.wait()
    gate[...] = rounded(contract(hidden[...], held[...])).astype(jnp.float32)


def attend_kernel(
    place,
    sink,
    queries,
    gate,
    low,
    middle,
    high,
    ctx,
    w_out,
    out,
    padded,
    mixed,
    held,
    ready,
    *,
    own,
    span,
):
    fetch = pltpu.make_async_copy(w_out, held, ready)
    fetch.start()
    rows = middle.shape[0]
    width = w_out.shape[0]
    heads = width // HEAD_SIZE
    padded[:WINDOW, :] = low[...].astype(jnp.float32)
    padded[WINDOW : WINDOW + rows, :] = middle[...].astype(jnp.float32)
    padded[WINDOW + rows : 2 * WINDOW + rows, :] = high[...].astype(jnp.float32)
    padded[2 * WINDOW + rows :, :] = jnp.zeros_like(padded[2 * WINDOW + rows :, :])
    row = lax.broadcasted_iota(jnp.int32, (own, span), 0)
    column = lax.broadcasted_iota(jnp.int32, (own, span), 1)
    in_reach = (column >= row) & (column <= row + 2 * WINDOW)
    lane = lax.broadcasted_iota(jnp.int32, (own, LANES), 1)
    sinks = jnp.concatenate([jnp.full((own, 1), sink[h], jnp.float32) for h in range(heads)], axis=0)
    blocks = rows // own
    for block in range(blocks):
        offset = pl.multiple_of(place[2 + block], 8)
        near = rounded(padded[pl.ds(offset, span), :])
        query = rounded(queries[block * heads * own : (block + 1) * heads * own, :])
        near_scores = contract(query, near, 1)
        ctx_scores = contract(query, ctx[...], 1)
        token = place[0] - WINDOW + offset + column
        seen = in_reach & (token >= 0) & (token < place[1])
        near_scores = jnp.where(
            seen[None], near_scores.reshape(heads, own, span), MASK_VALUE
        ).reshape(heads * own, span)
        peak = jnp.maximum(
            jnp.maximum(
                jnp.max(near_scores, axis=1, keepdims=True),
                jnp.max(ctx_scores, axis=1, keepdims=True),
            ),
            sinks,
        )
        near_exp = jnp.exp(near_scores - peak)
        ctx_exp = jnp.exp(ctx_scores - peak)
        denominator = (
            jnp.sum(near_exp, axis=1, keepdims=True)
            + jnp.sum(ctx_exp, axis=1, keepdims=True)
            + jnp.exp(sinks - peak)
        )
        inverse = 1.0 / denominator
        result = contract(rounded(near_exp * inverse), near) + contract(
            rounded(ctx_exp * inverse), ctx[...]
        )
        here = slice(block * own, (block + 1) * own)
        for pair in range(heads // 2):
            even = result[2 * pair * own : (2 * pair + 1) * own, :]
            odd = result[(2 * pair + 1) * own : (2 * pair + 2) * own, :]
            attended = jnp.where(lane < HEAD_SIZE, pltpu.roll(even, HEAD_SIZE, 1), odd)
            tile = gate[here, pair * LANES : (pair + 1) * LANES]
            mixed[here, pair * LANES : (pair + 1) * LANES] = attended * (
                tile / (1.0 + jnp.exp(-tile))
            )
    fetch.wait()
    final = rounded(mixed[...])
    step = 512
    for begin in range(0, w_out.shape[1], step):
        out[:, begin : begin + step] = rounded(contract(final, held[:, begin : begin + step]))


def copy_for_each(copies, axis):
    return lax.all_to_all(copies, axis, split_axis=0, concat_axis=0, tiled=True)


def shift(block, axis, steps, wrap=True):
    count = lax.axis_size(axis)
    pairs = [(i, (i + steps) % count) for i in range(count) if wrap or 0 <= i + steps < count]
    return lax.ppermute(block, axis, pairs)


def added(first, *others):
    total = first.astype(jnp.float32)
    for other in others:
        total = total + other.astype(jnp.float32)
    return rounded(total)


def toward(block, steps):
    tp_count, dp_count = lax.axis_size("tp"), lax.axis_size("dp")
    pairs = []
    for i in range(tp_count):
        for j in range(dp_count):
            target = (i + (steps if j % 2 == 0 else -steps)) % tp_count
            pairs.append((i * dp_count + j, target * dp_count + j))
    return lax.ppermute(block, ("tp", "dp"), pairs)


def gather_rows(latent):
    back2 = toward(latent, 2)
    ahead2 = toward(latent, -2)
    back1, ahead1 = toward(latent, 1), toward(latent, -1)
    far = toward(back2, 2)
    back3, ahead3 = toward(back2, 1), toward(ahead2, -1)
    return [(back3,), (back2,), (back1,), (latent,), (ahead1,), (ahead2,), (ahead3,), (far,)]


def reduce_rows(block):
    far = toward(block(4), 2)
    down3 = toward(block(-3), -1)
    up3 = toward(block(3), 1)
    minus_two = added(block(-2), down3)
    down2 = toward(minus_two, -2)
    ahead, _ = lax.optimization_barrier((block(2), minus_two))
    up2 = toward(added(ahead, up3, far), 2)
    up1, down1 = toward(block(1), 1), toward(block(-1), -1)
    total = block(0).astype(jnp.float32)
    for part in (up1, down1, up2, down2):
        total = total + part.astype(jnp.float32)
    return total


def angle_tables(positions):
    quarter = HEAD_SIZE // 4
    lane = jnp.arange(LANES, dtype=jnp.int32)
    entry = lane % (2 * quarter)
    exponent = (entry % quarter).astype(jnp.float32)
    inverse = jnp.exp(-math.log(10000.0) * exponent / quarter)
    grid_row = (positions // GRID_W).astype(jnp.float32)[:, None]
    grid_column = (positions % GRID_W).astype(jnp.float32)[:, None]
    angles = jnp.where(entry < quarter, grid_row, grid_column) * inverse
    sign = jnp.where(lane % HEAD_SIZE < HEAD_SIZE // 2, -1.0, 1.0)
    return jnp.cos(angles), jnp.sin(angles) * sign


def body(
    latent,
    condition,
    ctx_condition,
    context,
    mod_shift,
    mod_scale,
    mod_gate,
    norm_gain,
    w_query,
    key_weight,
    value_weight,
    w_gate,
    w_out,
    sink_logit,
):
    f32, bf16 = jnp.float32, jnp.bfloat16
    shape = jax.ShapeDtypeStruct
    sp_count, sp_rank = lax.axis_size("sp"), lax.axis_index("sp")
    tp_count, tp_rank = lax.axis_size("tp"), lax.axis_index("tp")
    own, width = latent.shape
    rows = own * tp_count
    mod_rows, columns = mod_shift.shape
    behind = (tp_count - 1) // 2

    parts = call(
        partial_kernel,
        shape((sp_count, 5, columns), f32),
        sp_rank.astype(jnp.int32)[None],
        condition,
        ctx_condition,
        mod_shift,
        mod_scale,
        mod_gate,
        specs=[SMEM, VMEM, VMEM, HBM, HBM, HBM],
        scratch=[pltpu.VMEM((3, mod_rows, columns), bf16), pltpu.SemaphoreType.DMA((3,))],
        grant=63,
    )
    pieces = gather_rows(latent)
    parts = copy_for_each(parts, "sp")
    totals = call(total_kernel, shape((tp_count, 5, columns), f32), parts)
    vectors = copy_for_each(totals, "tp")

    gain = norm_gain[None, :]
    kv_weight = jnp.concatenate([key_weight.T, value_weight.T], axis=0)
    direction = 1 - 2 * (lax.axis_index("dp") % 2)
    distance = jnp.arange(-behind, tp_count - behind, dtype=jnp.int32)
    offsets = (tp_rank + tp_count + direction * distance) % tp_count * own
    begin = sp_rank * rows
    positions = begin + (offsets[:, None] + jnp.arange(own, dtype=jnp.int32)).reshape(rows)
    cosine, sine = angle_tables(positions)
    place = jnp.concatenate([jnp.stack([begin, rows * sp_count]).astype(jnp.int32), offsets])

    ctx_rows = context.shape[0]
    ctx_pair = call(
        context_kernel,
        shape((sp_count, ctx_rows, LANES), bf16),
        context,
        vectors,
        gain,
        kv_weight,
        scratch=[pltpu.VMEM((ctx_rows, width), bf16)],
    )
    ctx_all = copy_for_each(ctx_pair, "sp").reshape(sp_count * ctx_rows, LANES)

    blocks = [block for piece in pieces for block in piece]
    hidden, key_value, first, last = call(
        functools.partial(key_kernel, pieces=[[0] * len(p) for p in pieces], per_group=2),
        [
            shape((rows, width), bf16),
            shape((rows, LANES), bf16),
            shape((WINDOW, LANES), bf16),
            shape((WINDOW, LANES), bf16),
        ],
        place,
        *blocks,
        vectors,
        gain,
        kv_weight,
        cosine,
        sine,
        specs=[SMEM] + [VMEM] * (len(blocks) + 5),
        scratch=[pltpu.VMEM((rows, LANES), f32)],
    )
    low = shift(last, "sp", 1, wrap=False)
    high = shift(first, "sp", -1, wrap=False)
    heads = w_query.shape[1] // HEAD_SIZE
    queries, gate = call(
        functools.partial(query_kernel, own=own),
        [shape((rows * heads, LANES), f32), shape((rows, w_gate.shape[1]), f32)],
        hidden,
        w_query,
        w_gate,
        cosine,
        sine,
        specs=[VMEM, VMEM, HBM, VMEM, VMEM],
        scratch=[pltpu.VMEM(w_gate.shape, bf16), pltpu.SemaphoreType.DMA],
        flops=2 * 10**9,
        grant=48,
    )
    span = 3 * LANES
    product = call(
        functools.partial(attend_kernel, own=own, span=span),
        shape((rows, width), bf16),
        place,
        sink_logit,
        queries,
        gate,
        low,
        key_value,
        high,
        ctx_all,
        w_out,
        specs=[SMEM, SMEM] + [VMEM] * 6 + [HBM],
        scratch=[
            pltpu.VMEM((rows - own + span, LANES), f32),
            pltpu.VMEM((rows, w_out.shape[0]), f32),
            pltpu.VMEM(w_out.shape, bf16),
            pltpu.SemaphoreType.DMA,
        ],
        flops=3 * 10**9,
        grant=50,
    )
    branch = reduce_rows(lambda d: product[(d + behind) * own : (d + behind + 1) * own])
    lat_gate = vectors[:, 4, :].reshape(width)
    return rounded(latent.astype(f32) + lat_gate * branch)


def solution(mesh):
    return jax.shard_map(
        body,
        mesh=mesh,
        in_specs=(
            P(("dp", "sp", "tp"), None),
            P("dp"),
            P(),
            P(("dp", "sp"), None),
            P("sp", "tp"),
            P("sp", "tp"),
            P("sp", "tp"),
            P(),
            P(None, "tp"),
            P(None, "tp"),
            P(None, "tp"),
            P(None, "tp"),
            P("tp", None),
            P("tp"),
        ),
        out_specs=P(("dp", "sp", "tp"), None),
        check_vma=False,
    )
```

```python
import functools
import math

import jax
import jax.numpy as jnp
from jax import lax
from jax.experimental import pallas as pl
from jax.experimental.pallas import tpu as pltpu
from jax.sharding import PartitionSpec as P

HEAD_SIZE = 64
WINDOW = 128
GRID_W = 64
LANES = 128
NORM_EPS = 1e-06
MASK_VALUE = -1e30
VMEM = pl.BlockSpec(memory_space=pltpu.VMEM)
HBM = pl.BlockSpec(memory_space=pltpu.HBM)
SMEM = pl.BlockSpec(memory_space=pltpu.SMEM)


def rounded(values):
    return values.astype(jnp.bfloat16)


def contract(left, right, right_dim=0):
    return lax.dot_general(
        left, right, (((1,), (right_dim,)), ((), ())), preferred_element_type=jnp.float32
    )


def call(kernel, out_shape, *operands, specs=None, scratch=(), flops=10**9, grant=30):
    return pl.pallas_call(
        kernel,
        out_shape=out_shape,
        in_specs=specs or [VMEM] * len(operands),
        out_specs=jax.tree.map(lambda _: VMEM, out_shape),
        scratch_shapes=scratch,
        compiler_params=pltpu.CompilerParams(vmem_limit_bytes=grant * 2**20),
        cost_estimate=pl.CostEstimate(flops=flops, bytes_accessed=10**6, transcendentals=0),
    )(*operands)


def row_offsets(own, count):
    direction = 1 - 2 * lax.rem(lax.axis_index("dp"), 2)
    rank = lax.axis_index("tp") + count
    behind = (count - 1) // 2
    return [
        lax.rem(rank + direction * distance, count) * own
        for distance in range(-behind, count - behind)
    ]


def partial_kernel(*refs, own):
    condition, ctx_condition, shift, scale, gate, out, cosine, sine = refs[:8]
    both, held, ready = refs[8:]
    fetches = [
        pltpu.make_async_copy(condition, both.at[0], ready.at[0]),
        pltpu.make_async_copy(ctx_condition, both.at[1], ready.at[1]),
    ]
    for index, weight in enumerate((shift, scale, gate)):
        fetches.append(pltpu.make_async_copy(weight, held.at[index], ready.at[2 + index]))
    for fetch in fetches:
        fetch.start()
    rows = cosine.shape[0]
    count = rows // own
    quarter = HEAD_SIZE // 4
    lane = lax.broadcasted_iota(jnp.int32, (own, LANES), 1)
    row = lax.broadcasted_iota(jnp.int32, (own, LANES), 0)
    entry = lane % (2 * quarter)
    inverse = jnp.exp(-math.log(10000.0) * (entry % quarter).astype(jnp.float32) / quarter)
    sign = jnp.where(lane % HEAD_SIZE < HEAD_SIZE // 2, -1.0, 1.0)
    begin = lax.axis_index("sp") * rows
    for index, offset in enumerate(row_offsets(own, count)):
        token = begin + offset + row
        angle = (
            jnp.where(entry < quarter, token // GRID_W, token % GRID_W).astype(jnp.float32)
            * inverse
        )
        cosine[index * own : (index + 1) * own, :] = jnp.cos(angle)
        sine[index * own : (index + 1) * own, :] = jnp.sin(angle) * sign
    for fetch in fetches[:2]:
        fetch.wait()
    size = held.shape[1]
    mine = pl.ds(pl.multiple_of(lax.axis_index("sp") * size, size), size)
    values = jnp.stack([both[0, mine], both[1, mine]])
    acts = rounded(values / (1.0 + jnp.exp(-values)))
    sums = []
    for index, fetch in enumerate(fetches[2:]):
        fetch.wait()
        sums.append(contract(acts, held[index]))
    sums = jnp.concatenate([sums[0], sums[1], sums[2][:1]], axis=0)
    for copy in range(out.shape[0]):
        out[copy] = sums


def total_kernel(parts, out):
    total = parts[0]
    for index in range(1, parts.shape[0]):
        total = total + parts[index]
    for copy in range(out.shape[0]):
        out[copy] = total


def modulated(pieces, vectors, gain, shift_row, scale_row, store):
    blocks, _, width = vectors.shape
    for read in pieces:
        square = None
        for block in range(blocks):
            values = read(block * width, width)
            part = sum(
                values[:, lane : lane + LANES] * values[:, lane : lane + LANES]
                for lane in range(0, width, LANES)
            )
            square = part if square is None else square + part
        mean = jnp.sum(square, axis=1, keepdims=True) / (blocks * width)
        inverse = lax.rsqrt(mean + NORM_EPS)
        for block in range(blocks):
            values = read(block * width, width)
            factor = gain[:, block * width : (block + 1) * width] * (
                1.0 + vectors[block, scale_row : scale_row + 1, :]
            )
            moved = values * inverse * factor + vectors[block, shift_row : shift_row + 1, :]
            store(read, block * width, rounded(moved))


def context_kernel(context, vectors, gain, key_weight, value_weight, out, hidden):
    def store(_, column, rows):
        hidden[:, column : column + rows.shape[1]] = rows

    modulated([lambda c, n: context[:, c : c + n].astype(jnp.float32)], vectors, gain, 1, 3, store)
    weight = jnp.concatenate([key_weight[...], value_weight[...]], axis=0)
    pair = rounded(contract(hidden[...], weight, 1))
    for copy in range(out.shape[0]):
        out[copy] = pair


def turned(values, cosine, sine):
    lane = lax.broadcasted_iota(jnp.int32, values.shape, 1)
    half = HEAD_SIZE // 2
    other = jnp.where(
        lane % HEAD_SIZE < half, pltpu.roll(values, LANES - half, 1), pltpu.roll(values, half, 1)
    )
    return values * cosine + other * sine


def key_kernel(*refs, pieces, per_group):
    count = sum(len(piece) for piece in pieces)
    blocks = list(refs[:count])
    vectors, gain, key_weight, value_weight, cosine, sine = refs[count : 6 + count]
    hidden, key_value, first, last, ordered = refs[6 + count :]
    own = hidden.shape[0] // len(pieces)
    members = [[blocks.pop(0) for _ in piece] for piece in pieces]
    reads, places = [], {}
    for group in range(0, len(members), per_group):

        def read(column, columns, parts=members[group : group + per_group]):
            rows = []
            for part in parts:
                held = part[0].shape[1]
                ref, at = part[column // held], column % held
                rows.append(ref[:, at : at + columns].astype(jnp.float32))
            return jnp.concatenate(rows, axis=0) if len(rows) > 1 else rows[0]

        reads.append(read)
        places[read] = group * own

    def store(read, column, rows):
        begin = places[read]
        hidden[begin : begin + rows.shape[0], column : column + rows.shape[1]] = rows

    modulated(reads, vectors, gain, 0, 2, store)
    weight = jnp.concatenate([key_weight[...], value_weight[...]], axis=0)
    both = contract(hidden[...], weight, 1)
    lane = lax.broadcasted_iota(jnp.int32, both.shape, 1)
    both = jnp.where(lane < HEAD_SIZE, turned(both, cosine[...], sine[...]), both)
    for index, offset in enumerate(row_offsets(own, len(pieces))):
        begin = pl.multiple_of(offset, 8)
        ordered[pl.ds(begin, own), :] = both[index * own : (index + 1) * own, :]
    key_value[...] = rounded(ordered[...])
    first[...] = rounded(ordered[:WINDOW, :])
    last[...] = rounded(ordered[ordered.shape[0] - WINDOW :, :])


def query_kernel(hidden, w_query, w_gate, cosine, sine, queries, gate, held, ready, *, own):
    fetch = pltpu.make_async_copy(w_gate, held, ready)
    fetch.start()
    rows, width = hidden.shape[0], w_query.shape[1]
    projected = contract(hidden[...], w_query[...])
    heads = width // HEAD_SIZE
    lane = lax.broadcasted_iota(jnp.int32, (rows, LANES), 1)
    for pair in range(width // LANES):
        tile = turned(projected[:, pair * LANES : (pair + 1) * LANES], cosine[...], sine[...])
        tile = tile * (1.0 / math.sqrt(HEAD_SIZE))
        for odd in range(2):
            head = 2 * pair + odd
            aligned = pltpu.roll(tile, HEAD_SIZE, 1) if odd else tile
            aligned = jnp.where(lane < HEAD_SIZE, aligned, 0.0)
            for block in range(rows // own):
                begin = (block * heads + head) * own
                queries[begin : begin + own, :] = aligned[block * own : (block + 1) * own, :]
    fetch.wait()
    gate[...] = rounded(contract(hidden[...], held[...])).astype(jnp.float32)


def attend_kernel(
    sink,
    queries,
    gate,
    low,
    middle,
    high,
    ctx,
    w_out,
    out,
    padded,
    mixed,
    held,
    ready,
    *,
    own,
    span,
):
    fetch = pltpu.make_async_copy(w_out, held, ready)
    fetch.start()
    rows = middle.shape[0]
    width = w_out.shape[0]
    heads = width // HEAD_SIZE
    padded[:WINDOW, :] = low[...].astype(jnp.float32)
    padded[WINDOW : WINDOW + rows, :] = middle[...].astype(jnp.float32)
    padded[WINDOW + rows : 2 * WINDOW + rows, :] = high[...].astype(jnp.float32)
    padded[2 * WINDOW + rows :, :] = jnp.zeros_like(padded[2 * WINDOW + rows :, :])
    row = lax.broadcasted_iota(jnp.int32, (own, span), 0)
    column = lax.broadcasted_iota(jnp.int32, (own, span), 1)
    in_reach = (column >= row) & (column <= row + 2 * WINDOW)
    lane = lax.broadcasted_iota(jnp.int32, (own, LANES), 1)
    sinks = jnp.concatenate([jnp.full((own, 1), sink[h], jnp.float32) for h in range(heads)], axis=0)
    begin = lax.axis_index("sp") * rows
    total = lax.axis_size("sp") * rows
    for block, offset in enumerate(row_offsets(own, rows // own)):
        offset = pl.multiple_of(offset, 8)
        near = rounded(padded[pl.ds(offset, span), :])
        query = rounded(queries[block * heads * own : (block + 1) * heads * own, :])
        near_scores = contract(query, near, 1)
        ctx_scores = contract(query, ctx[...], 1)
        token = begin - WINDOW + offset + column
        seen = in_reach & (token >= 0) & (token < total)
        near_scores = jnp.where(
            seen[None], near_scores.reshape(heads, own, span), MASK_VALUE
        ).reshape(heads * own, span)
        peak = jnp.maximum(
            jnp.maximum(
                jnp.max(near_scores, axis=1, keepdims=True),
                jnp.max(ctx_scores, axis=1, keepdims=True),
            ),
            sinks,
        )
        near_exp = jnp.exp(near_scores - peak)
        ctx_exp = jnp.exp(ctx_scores - peak)
        denominator = (
            jnp.sum(near_exp, axis=1, keepdims=True)
            + jnp.sum(ctx_exp, axis=1, keepdims=True)
            + jnp.exp(sinks - peak)
        )
        inverse = 1.0 / denominator
        result = contract(rounded(near_exp * inverse), near) + contract(
            rounded(ctx_exp * inverse), ctx[...]
        )
        here = slice(block * own, (block + 1) * own)
        for pair in range(heads // 2):
            even = result[2 * pair * own : (2 * pair + 1) * own, :]
            odd = result[(2 * pair + 1) * own : (2 * pair + 2) * own, :]
            attended = jnp.where(lane < HEAD_SIZE, pltpu.roll(even, HEAD_SIZE, 1), odd)
            tile = gate[here, pair * LANES : (pair + 1) * LANES]
            mixed[here, pair * LANES : (pair + 1) * LANES] = attended * (
                tile / (1.0 + jnp.exp(-tile))
            )
    fetch.wait()
    final = rounded(mixed[...])
    step = 512
    for begin in range(0, w_out.shape[1], step):
        out[:, begin : begin + step] = rounded(contract(final, held[:, begin : begin + step]))


def copy_for_each(copies, axis):
    return lax.all_to_all(copies, axis, split_axis=0, concat_axis=0, tiled=True)


def shift(block, axis, steps, wrap=True):
    count = lax.axis_size(axis)
    pairs = [(i, (i + steps) % count) for i in range(count) if wrap or 0 <= i + steps < count]
    return lax.ppermute(block, axis, pairs)


def added(first, *others):
    total = first.astype(jnp.float32)
    for other in others:
        total = total + other.astype(jnp.float32)
    return rounded(total)


def toward(block, steps):
    tp_count, dp_count = lax.axis_size("tp"), lax.axis_size("dp")
    pairs = []
    for i in range(tp_count):
        for j in range(dp_count):
            target = (i + (steps if j % 2 == 0 else -steps)) % tp_count
            pairs.append((i * dp_count + j, target * dp_count + j))
    return lax.ppermute(block, ("tp", "dp"), pairs)


def gather_rows(latent):
    back2 = toward(latent, 2)
    ahead2 = toward(latent, -2)
    back1 = toward(latent, 1)
    ahead1 = toward(latent, -1)
    far = toward(back2, 2)
    back3, ahead3 = toward(back2, 1), toward(ahead2, -1)
    return [(back3,), (back2,), (back1,), (latent,), (ahead1,), (ahead2,), (ahead3,), (far,)]


def reduce_rows(block):
    far = toward(block(4), 2)
    down3 = toward(block(-3), -1)
    up3 = toward(block(3), 1)
    minus_two = added(block(-2), down3)
    down2 = toward(minus_two, -2)
    ahead, _ = lax.optimization_barrier((block(2), minus_two))
    up2 = toward(added(ahead, up3, far), 2)
    up1 = toward(block(1), 1)
    down1 = toward(block(-1), -1)
    total = block(0).astype(jnp.float32)
    for part in (up1, down1, up2, down2):
        total = total + part.astype(jnp.float32)
    return total


def body(
    latent,
    condition,
    ctx_condition,
    context,
    mod_shift,
    mod_scale,
    mod_gate,
    norm_gain,
    w_query,
    key_weight,
    value_weight,
    w_gate,
    w_out,
    sink_logit,
):
    f32, bf16 = jnp.float32, jnp.bfloat16
    shape = jax.ShapeDtypeStruct
    sp_count, tp_count = lax.axis_size("sp"), lax.axis_size("tp")
    own, width = latent.shape
    rows = own * tp_count
    mod_rows, columns = mod_shift.shape
    behind = (tp_count - 1) // 2

    parts, cosine, sine = call(
        functools.partial(partial_kernel, own=own),
        [
            shape((sp_count, 5, columns), f32),
            shape((rows, LANES), f32),
            shape((rows, LANES), f32),
        ],
        condition,
        ctx_condition,
        mod_shift,
        mod_scale,
        mod_gate,
        specs=[HBM] * 5,
        scratch=[
            pltpu.VMEM((2, *condition.shape), f32),
            pltpu.VMEM((3, mod_rows, columns), bf16),
            pltpu.SemaphoreType.DMA((5,)),
        ],
        grant=62,
    )
    pieces = gather_rows(latent)
    parts = copy_for_each(parts, "sp")
    totals = call(total_kernel, shape((tp_count, 5, columns), f32), parts, grant=30)
    vectors = copy_for_each(totals, "tp")

    gain = norm_gain[None, :]
    kv_weights = (key_weight.T, value_weight.T)
    ctx_rows = context.shape[0]
    ctx_pair = call(
        context_kernel,
        shape((sp_count, ctx_rows, LANES), bf16),
        context,
        vectors,
        gain,
        *kv_weights,
        scratch=[pltpu.VMEM((ctx_rows, width), bf16)],
        grant=30,
    )
    ctx_all = copy_for_each(ctx_pair, "sp").reshape(sp_count * ctx_rows, LANES)

    blocks = [block for piece in pieces for block in piece]
    hidden, key_value, first, last = call(
        functools.partial(key_kernel, pieces=[[0] * len(p) for p in pieces], per_group=2),
        [
            shape((rows, width), bf16),
            shape((rows, LANES), bf16),
            shape((WINDOW, LANES), bf16),
            shape((WINDOW, LANES), bf16),
        ],
        *blocks,
        vectors,
        gain,
        *kv_weights,
        cosine,
        sine,
        scratch=[pltpu.VMEM((rows, LANES), f32)],
        grant=30,
    )
    low = shift(last, "sp", 1, wrap=False)
    high = shift(first, "sp", -1, wrap=False)
    heads = w_query.shape[1] // HEAD_SIZE
    queries, gate = call(
        functools.partial(query_kernel, own=own),
        [shape((rows * heads, LANES), f32), shape((rows, w_gate.shape[1]), f32)],
        hidden,
        w_query,
        w_gate,
        cosine,
        sine,
        specs=[VMEM, VMEM, HBM, VMEM, VMEM],
        scratch=[pltpu.VMEM(w_gate.shape, bf16), pltpu.SemaphoreType.DMA],
        flops=2 * 10**9,
        grant=46,
    )
    span = 3 * LANES
    product = call(
        functools.partial(attend_kernel, own=own, span=span),
        shape((rows, width), bf16),
        sink_logit,
        queries,
        gate,
        low,
        key_value,
        high,
        ctx_all,
        w_out,
        specs=[SMEM] + [VMEM] * 6 + [HBM],
        scratch=[
            pltpu.VMEM((rows - own + span, LANES), f32),
            pltpu.VMEM((rows, w_out.shape[0]), f32),
            pltpu.VMEM(w_out.shape, bf16),
            pltpu.SemaphoreType.DMA,
        ],
        flops=3 * 10**9,
        grant=50,
    )
    branch = reduce_rows(lambda d: product[(d + behind) * own : (d + behind + 1) * own])
    lat_gate = vectors[:, 4, :].reshape(width)
    return rounded(latent.astype(f32) + lat_gate * branch)


def solution(mesh):
    return jax.shard_map(
        body,
        mesh=mesh,
        in_specs=(
            P(("dp", "sp", "tp"), None),
            P("dp"),
            P(),
            P(("dp", "sp"), None),
            P("sp", "tp"),
            P("sp", "tp"),
            P("sp", "tp"),
            P(),
            P(None, "tp"),
            P(None, "tp"),
            P(None, "tp"),
            P(None, "tp"),
            P("tp", None),
            P("tp"),
        ),
        out_specs=P(("dp", "sp", "tp"), None),
        check_vma=False,
    )
```

```python
import functools
import math

import jax
import jax.numpy as jnp
from jax import lax
from jax.experimental import pallas as pl
from jax.experimental.pallas import tpu as pltpu
from jax.sharding import PartitionSpec as P

HEAD_SIZE = 64
WINDOW = 128
GRID_W = 64
LANES = 128
NORM_EPS = 1e-06
MASK_VALUE = -1e30
VMEM = pl.BlockSpec(memory_space=pltpu.VMEM)
HBM = pl.BlockSpec(memory_space=pltpu.HBM)
SMEM = pl.BlockSpec(memory_space=pltpu.SMEM)


def rounded(values):
    return values.astype(jnp.bfloat16)


def contract(left, right, right_dim=0):
    return lax.dot_general(
        left, right, (((1,), (right_dim,)), ((), ())), preferred_element_type=jnp.float32
    )


def call(kernel, out_shape, *operands, specs=None, scratch=(), flops=10**9, grant=30):
    return pl.pallas_call(
        kernel,
        out_shape=out_shape,
        in_specs=specs or [VMEM] * len(operands),
        out_specs=jax.tree.map(lambda _: VMEM, out_shape),
        scratch_shapes=scratch,
        compiler_params=pltpu.CompilerParams(vmem_limit_bytes=grant * 2**20),
        cost_estimate=pl.CostEstimate(flops=flops, bytes_accessed=10**6, transcendentals=0),
    )(*operands)


def row_offsets(own, count):
    direction = 1 - 2 * lax.rem(lax.axis_index("dp"), 2)
    rank = lax.axis_index("tp") + count
    behind = (count - 1) // 2
    return [
        lax.rem(rank + direction * distance, count) * own
        for distance in range(-behind, count - behind)
    ]


def partial_kernel(*refs, own):
    condition, ctx_condition, shift, scale, gate, out, cosine, sine = refs[:8]
    both, held, ready = refs[8:]
    fetches = [
        pltpu.make_async_copy(condition, both.at[0], ready.at[0]),
        pltpu.make_async_copy(ctx_condition, both.at[1], ready.at[1]),
    ]
    for index, weight in enumerate((shift, scale, gate)):
        fetches.append(pltpu.make_async_copy(weight, held.at[index], ready.at[2 + index]))
    for fetch in fetches:
        fetch.start()
    rows = cosine.shape[0]
    count = rows // own
    quarter = HEAD_SIZE // 4
    lane = lax.broadcasted_iota(jnp.int32, (own, LANES), 1)
    row = lax.broadcasted_iota(jnp.int32, (own, LANES), 0)
    entry = lane % (2 * quarter)
    inverse = jnp.exp(-math.log(10000.0) * (entry % quarter).astype(jnp.float32) / quarter)
    sign = jnp.where(lane % HEAD_SIZE < HEAD_SIZE // 2, -1.0, 1.0)
    begin = lax.axis_index("sp") * rows
    for index, offset in enumerate(row_offsets(own, count)):
        token = begin + offset + row
        angle = (
            jnp.where(entry < quarter, token // GRID_W, token % GRID_W).astype(jnp.float32)
            * inverse
        )
        cosine[index * own : (index + 1) * own, :] = jnp.cos(angle)
        sine[index * own : (index + 1) * own, :] = jnp.sin(angle) * sign
    for fetch in fetches[:2]:
        fetch.wait()
    size = held.shape[1]
    mine = pl.ds(pl.multiple_of(lax.axis_index("sp") * size, size), size)
    values = jnp.stack([both[0, mine], both[1, mine]])
    acts = rounded(values / (1.0 + jnp.exp(-values)))
    sums = []
    for index, fetch in enumerate(fetches[2:]):
        fetch.wait()
        sums.append(contract(acts, held[index]))
    sums = jnp.concatenate([sums[0], sums[1], sums[2][:1]], axis=0)
    for copy in range(out.shape[0]):
        out[copy] = sums


def total_kernel(parts, out):
    total = parts[0]
    for index in range(1, parts.shape[0]):
        total = total + parts[index]
    for copy in range(out.shape[0]):
        out[copy] = total


def modulated(pieces, vectors, gain, shift_row, scale_row, store):
    blocks, _, width = vectors.shape
    for read in pieces:
        square = None
        for block in range(blocks):
            values = read(block * width, width)
            part = sum(
                values[:, lane : lane + LANES] * values[:, lane : lane + LANES]
                for lane in range(0, width, LANES)
            )
            square = part if square is None else square + part
        mean = jnp.sum(square, axis=1, keepdims=True) / (blocks * width)
        inverse = lax.rsqrt(mean + NORM_EPS)
        for block in range(blocks):
            values = read(block * width, width)
            factor = gain[:, block * width : (block + 1) * width] * (
                1.0 + vectors[block, scale_row : scale_row + 1, :]
            )
            moved = values * inverse * factor + vectors[block, shift_row : shift_row + 1, :]
            store(read, block * width, rounded(moved))


def context_kernel(context, vectors, gain, key_weight, value_weight, out, hidden):
    def store(_, column, rows):
        hidden[:, column : column + rows.shape[1]] = rows

    modulated([lambda c, n: context[:, c : c + n].astype(jnp.float32)], vectors, gain, 1, 3, store)
    weight = jnp.concatenate([key_weight[...], value_weight[...]], axis=0)
    pair = rounded(contract(hidden[...], weight, 1))
    for copy in range(out.shape[0]):
        out[copy] = pair


def turned(values, cosine, sine):
    lane = lax.broadcasted_iota(jnp.int32, values.shape, 1)
    half = HEAD_SIZE // 2
    other = jnp.where(
        lane % HEAD_SIZE < half, pltpu.roll(values, LANES - half, 1), pltpu.roll(values, half, 1)
    )
    return values * cosine + other * sine


def key_kernel(*refs, pieces, per_group):
    count = sum(len(piece) for piece in pieces)
    blocks = list(refs[:count])
    vectors, gain, key_weight, value_weight, cosine, sine = refs[count : 6 + count]
    hidden, key_value, first, last, ordered = refs[6 + count :]
    own = hidden.shape[0] // len(pieces)
    members = [[blocks.pop(0) for _ in piece] for piece in pieces]
    reads, places = [], {}
    for group in range(0, len(members), per_group):

        def read(column, columns, parts=members[group : group + per_group]):
            rows = []
            for part in parts:
                held = part[0].shape[1]
                ref, at = part[column // held], column % held
                rows.append(ref[:, at : at + columns].astype(jnp.float32))
            return jnp.concatenate(rows, axis=0) if len(rows) > 1 else rows[0]

        reads.append(read)
        places[read] = group * own

    def store(read, column, rows):
        begin = places[read]
        hidden[begin : begin + rows.shape[0], column : column + rows.shape[1]] = rows

    modulated(reads, vectors, gain, 0, 2, store)
    weight = jnp.concatenate([key_weight[...], value_weight[...]], axis=0)
    both = contract(hidden[...], weight, 1)
    lane = lax.broadcasted_iota(jnp.int32, both.shape, 1)
    both = jnp.where(lane < HEAD_SIZE, turned(both, cosine[...], sine[...]), both)
    for index, offset in enumerate(row_offsets(own, len(pieces))):
        begin = pl.multiple_of(offset, 8)
        ordered[pl.ds(begin, own), :] = both[index * own : (index + 1) * own, :]
    key_value[...] = rounded(ordered[...])
    first[...] = rounded(ordered[:WINDOW, :])
    last[...] = rounded(ordered[ordered.shape[0] - WINDOW :, :])


def query_kernel(hidden, w_query, w_gate, cosine, sine, queries, gate, held, ready, *, own):
    fetch = pltpu.make_async_copy(w_gate, held, ready)
    fetch.start()
    rows, width = hidden.shape[0], w_query.shape[1]
    projected = contract(hidden[...], w_query[...])
    heads = width // HEAD_SIZE
    lane = lax.broadcasted_iota(jnp.int32, (rows, LANES), 1)
    for pair in range(width // LANES):
        tile = turned(projected[:, pair * LANES : (pair + 1) * LANES], cosine[...], sine[...])
        tile = tile * (1.0 / math.sqrt(HEAD_SIZE))
        for odd in range(2):
            head = 2 * pair + odd
            aligned = pltpu.roll(tile, HEAD_SIZE, 1) if odd else tile
            aligned = jnp.where(lane < HEAD_SIZE, aligned, 0.0)
            for block in range(rows // own):
                begin = (block * heads + head) * own
                queries[begin : begin + own, :] = aligned[block * own : (block + 1) * own, :]
    fetch.wait()
    gate[...] = rounded(contract(hidden[...], held[...])).astype(jnp.float32)


def attend_kernel(
    sink,
    queries,
    gate,
    low,
    middle,
    high,
    ctx,
    w_out,
    out,
    padded,
    mixed,
    held,
    ready,
    *,
    own,
    span,
):
    fetch = pltpu.make_async_copy(w_out, held, ready)
    fetch.start()
    rows = middle.shape[0]
    width = w_out.shape[0]
    heads = width // HEAD_SIZE
    padded[:WINDOW, :] = low[...].astype(jnp.float32)
    padded[WINDOW : WINDOW + rows, :] = middle[...].astype(jnp.float32)
    padded[WINDOW + rows : 2 * WINDOW + rows, :] = high[...].astype(jnp.float32)
    padded[2 * WINDOW + rows :, :] = jnp.zeros_like(padded[2 * WINDOW + rows :, :])
    row = lax.broadcasted_iota(jnp.int32, (own, span), 0)
    column = lax.broadcasted_iota(jnp.int32, (own, span), 1)
    in_reach = (column >= row) & (column <= row + 2 * WINDOW)
    lane = lax.broadcasted_iota(jnp.int32, (own, LANES), 1)
    sinks = jnp.concatenate([jnp.full((own, 1), sink[h], jnp.float32) for h in range(heads)], axis=0)
    begin = lax.axis_index("sp") * rows
    total = lax.axis_size("sp") * rows
    offsets = row_offsets(own, rows // own)

    def scored(block):
        offset = pl.multiple_of(offsets[block], 8)
        keys = jnp.concatenate([rounded(padded[pl.ds(offset, span), :]), ctx[...]], axis=0)
        query = rounded(queries[block * heads * own : (block + 1) * heads * own, :])
        scores = contract(query, keys, 1)
        token = begin - WINDOW + offset + column
        seen = in_reach & (token >= 0) & (token < total)
        near = jnp.where(seen[None], scores[:, :span].reshape(heads, own, span), MASK_VALUE)
        scores = jnp.concatenate([near.reshape(heads * own, span), scores[:, span:]], axis=1)
        return scores, keys

    following = scored(0)
    for block in range(rows // own):
        scores, keys = following
        if block + 1 < rows // own:
            following = scored(block + 1)
        peak = jnp.maximum(jnp.max(scores, axis=1, keepdims=True), sinks)
        weights = jnp.exp(scores - peak)
        denominator = jnp.sum(weights, axis=1, keepdims=True) + jnp.exp(sinks - peak)
        result = contract(rounded(weights), keys) * (1.0 / denominator)
        here = slice(block * own, (block + 1) * own)
        for pair in range(heads // 2):
            even = result[2 * pair * own : (2 * pair + 1) * own, :]
            odd = result[(2 * pair + 1) * own : (2 * pair + 2) * own, :]
            attended = jnp.where(lane < HEAD_SIZE, pltpu.roll(even, HEAD_SIZE, 1), odd)
            tile = gate[here, pair * LANES : (pair + 1) * LANES]
            mixed[here, pair * LANES : (pair + 1) * LANES] = attended * (
                tile / (1.0 + jnp.exp(-tile))
            )
    fetch.wait()
    final = rounded(mixed[...])
    step = 512
    for begin in range(0, w_out.shape[1], step):
        out[:, begin : begin + step] = rounded(contract(final, held[:, begin : begin + step]))


def copy_for_each(copies, axis):
    return lax.all_to_all(copies, axis, split_axis=0, concat_axis=0, tiled=True)


def shift(block, axis, steps, wrap=True):
    count = lax.axis_size(axis)
    pairs = [(i, (i + steps) % count) for i in range(count) if wrap or 0 <= i + steps < count]
    return lax.ppermute(block, axis, pairs)


def added(first, *others):
    total = first.astype(jnp.float32)
    for other in others:
        total = total + other.astype(jnp.float32)
    return rounded(total)


def toward(block, steps):
    tp_count, dp_count = lax.axis_size("tp"), lax.axis_size("dp")
    pairs = []
    for i in range(tp_count):
        for j in range(dp_count):
            target = (i + (steps if j % 2 == 0 else -steps)) % tp_count
            pairs.append((i * dp_count + j, target * dp_count + j))
    return lax.ppermute(block, ("tp", "dp"), pairs)


def gather_rows(latent):
    ahead2 = toward(latent, -2)
    ahead1 = toward(latent, -1)
    back2 = toward(latent, 2)
    back1 = toward(latent, 1)
    far = toward(back2, 2)
    back3 = toward(back2, 1)
    ahead3 = toward(ahead2, -1)
    return [(back3,), (back2,), (back1,), (latent,), (ahead1,), (ahead2,), (ahead3,), (far,)]


def reduce_rows(block):
    far = toward(block(4), 2)
    up3 = toward(block(3), 1)
    down3 = toward(block(-3), -1)
    down1 = toward(block(-1), -1)
    two = added(block(2), up3, far)
    up2 = toward(two, 2)
    up1 = toward(block(1), 1)
    behind, _ = lax.optimization_barrier((block(-2), two))
    down2 = toward(added(behind, down3), -2)
    total = block(0).astype(jnp.float32)
    for part in (up1, down1, up2, down2):
        total = total + part.astype(jnp.float32)
    return total


def body(
    latent,
    condition,
    ctx_condition,
    context,
    mod_shift,
    mod_scale,
    mod_gate,
    norm_gain,
    w_query,
    key_weight,
    value_weight,
    w_gate,
    w_out,
    sink_logit,
):
    f32, bf16 = jnp.float32, jnp.bfloat16
    shape = jax.ShapeDtypeStruct
    sp_count, tp_count = lax.axis_size("sp"), lax.axis_size("tp")
    own, width = latent.shape
    rows = own * tp_count
    mod_rows, columns = mod_shift.shape
    behind = (tp_count - 1) // 2

    parts, cosine, sine = call(
        functools.partial(partial_kernel, own=own),
        [
            shape((sp_count, 5, columns), f32),
            shape((rows, LANES), f32),
            shape((rows, LANES), f32),
        ],
        condition,
        ctx_condition,
        mod_shift,
        mod_scale,
        mod_gate,
        specs=[HBM] * 5,
        scratch=[
            pltpu.VMEM((2, *condition.shape), f32),
            pltpu.VMEM((3, mod_rows, columns), bf16),
            pltpu.SemaphoreType.DMA((5,)),
        ],
        grant=62,
    )
    pieces = gather_rows(latent)
    parts = copy_for_each(parts, "sp")
    totals = call(total_kernel, shape((tp_count, 5, columns), f32), parts, grant=30)
    vectors = copy_for_each(totals, "tp")

    gain = norm_gain[None, :]
    kv_weights = (key_weight.T, value_weight.T)
    ctx_rows = context.shape[0]
    ctx_pair = call(
        context_kernel,
        shape((sp_count, ctx_rows, LANES), bf16),
        context,
        vectors,
        gain,
        *kv_weights,
        scratch=[pltpu.VMEM((ctx_rows, width), bf16)],
        grant=30,
    )
    ctx_all = copy_for_each(ctx_pair, "sp").reshape(sp_count * ctx_rows, LANES)

    blocks = [block for piece in pieces for block in piece]
    hidden, key_value, first, last = call(
        functools.partial(key_kernel, pieces=[[0] * len(p) for p in pieces], per_group=2),
        [
            shape((rows, width), bf16),
            shape((rows, LANES), bf16),
            shape((WINDOW, LANES), bf16),
            shape((WINDOW, LANES), bf16),
        ],
        *blocks,
        vectors,
        gain,
        *kv_weights,
        cosine,
        sine,
        scratch=[pltpu.VMEM((rows, LANES), f32)],
        grant=30,
    )
    low = shift(last, "sp", 1, wrap=False)
    high = shift(first, "sp", -1, wrap=False)
    heads = w_query.shape[1] // HEAD_SIZE
    queries, gate = call(
        functools.partial(query_kernel, own=own),
        [shape((rows * heads, LANES), f32), shape((rows, w_gate.shape[1]), f32)],
        hidden,
        w_query,
        w_gate,
        cosine,
        sine,
        specs=[VMEM, VMEM, HBM, VMEM, VMEM],
        scratch=[pltpu.VMEM(w_gate.shape, bf16), pltpu.SemaphoreType.DMA],
        flops=2 * 10**9,
        grant=46,
    )
    span = 3 * LANES
    product = call(
        functools.partial(attend_kernel, own=own, span=span),
        shape((rows, width), bf16),
        sink_logit,
        queries,
        gate,
        low,
        key_value,
        high,
        ctx_all,
        w_out,
        specs=[SMEM] + [VMEM] * 6 + [HBM],
        scratch=[
            pltpu.VMEM((rows - own + span, LANES), f32),
            pltpu.VMEM((rows, w_out.shape[0]), f32),
            pltpu.VMEM(w_out.shape, bf16),
            pltpu.SemaphoreType.DMA,
        ],
        flops=3 * 10**9,
        grant=50,
    )
    branch = reduce_rows(lambda d: product[(d + behind) * own : (d + behind + 1) * own])
    lat_gate = vectors[:, 4, :].reshape(width)
    return rounded(latent.astype(f32) + lat_gate * branch)


def solution(mesh):
    return jax.shard_map(
        body,
        mesh=mesh,
        in_specs=(
            P(("dp", "sp", "tp"), None),
            P("dp"),
            P(),
            P(("dp", "sp"), None),
            P("sp", "tp"),
            P("sp", "tp"),
            P("sp", "tp"),
            P(),
            P(None, "tp"),
            P(None, "tp"),
            P(None, "tp"),
            P(None, "tp"),
            P("tp", None),
            P("tp"),
        ),
        out_specs=P(("dp", "sp", "tp"), None),
        check_vma=False,
    )
```

```python
import functools
import math

import jax
import jax.numpy as jnp
from jax import lax
from jax.experimental import pallas as pl
from jax.experimental.pallas import tpu as pltpu
from jax.sharding import PartitionSpec as P

HEAD_SIZE = 64
WINDOW = 128
GRID_W = 64
LANES = 128
NORM_EPS = 1e-06
MASK_VALUE = -1e30
VMEM = pl.BlockSpec(memory_space=pltpu.VMEM)
HBM = pl.BlockSpec(memory_space=pltpu.HBM)
SMEM = pl.BlockSpec(memory_space=pltpu.SMEM)


def rounded(values):
    return values.astype(jnp.bfloat16)


def contract(left, right, right_dim=0):
    return lax.dot_general(
        left, right, (((1,), (right_dim,)), ((), ())), preferred_element_type=jnp.float32
    )


def call(kernel, out_shape, *operands, specs=None, scratch=(), flops=10**9, grant=30):
    return pl.pallas_call(
        kernel,
        out_shape=out_shape,
        in_specs=specs or [VMEM] * len(operands),
        out_specs=jax.tree.map(lambda _: VMEM, out_shape),
        scratch_shapes=scratch,
        compiler_params=pltpu.CompilerParams(vmem_limit_bytes=grant * 2**20),
        cost_estimate=pl.CostEstimate(flops=flops, bytes_accessed=10**6, transcendentals=0),
    )(*operands)


def row_offsets(own, count):
    direction = 1 - 2 * lax.rem(lax.axis_index("dp"), 2)
    rank = lax.axis_index("tp") + count
    behind = (count - 1) // 2
    return [
        lax.rem(rank + direction * distance, count) * own
        for distance in range(-behind, count - behind)
    ]


def partial_kernel(*refs, own):
    condition, ctx_condition, shift, scale, gate, out, cosine, sine = refs[:8]
    both, held, ready = refs[8:]
    fetches = [
        pltpu.make_async_copy(condition, both.at[0], ready.at[0]),
        pltpu.make_async_copy(ctx_condition, both.at[1], ready.at[1]),
    ]
    for index, weight in enumerate((shift, scale, gate)):
        fetches.append(pltpu.make_async_copy(weight, held.at[index], ready.at[2 + index]))
    for fetch in fetches:
        fetch.start()
    rows = cosine.shape[0]
    count = rows // own
    quarter = HEAD_SIZE // 4
    lane = lax.broadcasted_iota(jnp.int32, (own, LANES), 1)
    row = lax.broadcasted_iota(jnp.int32, (own, LANES), 0)
    entry = lane % (2 * quarter)
    inverse = jnp.exp(-math.log(10000.0) * (entry % quarter).astype(jnp.float32) / quarter)
    sign = jnp.where(lane % HEAD_SIZE < HEAD_SIZE // 2, -1.0, 1.0)
    begin = lax.axis_index("sp") * rows
    for index, offset in enumerate(row_offsets(own, count)):
        token = begin + offset + row
        angle = (
            jnp.where(entry < quarter, token // GRID_W, token % GRID_W).astype(jnp.float32)
            * inverse
        )
        cosine[index * own : (index + 1) * own, :] = jnp.cos(angle)
        sine[index * own : (index + 1) * own, :] = jnp.sin(angle) * sign
    for fetch in fetches[:2]:
        fetch.wait()
    size = held.shape[1]
    mine = pl.ds(pl.multiple_of(lax.axis_index("sp") * size, size), size)
    values = jnp.stack([both[0, mine], both[1, mine]])
    acts = rounded(values / (1.0 + jnp.exp(-values)))
    sums = []
    for index, fetch in enumerate(fetches[2:]):
        fetch.wait()
        sums.append(contract(acts, held[index]))
    sums = jnp.concatenate([sums[0], sums[1], sums[2][:1]], axis=0)
    for copy in range(out.shape[0]):
        out[copy] = sums


def total_kernel(parts, out):
    total = parts[0]
    for index in range(1, parts.shape[0]):
        total = total + parts[index]
    for copy in range(out.shape[0]):
        out[copy] = total


def modulated(pieces, vectors, gain, shift_row, scale_row, store):
    blocks, _, width = vectors.shape
    for read in pieces:
        square = None
        for block in range(blocks):
            values = read(block * width, width)
            part = sum(
                values[:, lane : lane + LANES] * values[:, lane : lane + LANES]
                for lane in range(0, width, LANES)
            )
            square = part if square is None else square + part
        mean = jnp.sum(square, axis=1, keepdims=True) / (blocks * width)
        inverse = lax.rsqrt(mean + NORM_EPS)
        for block in range(blocks):
            values = read(block * width, width)
            factor = gain[:, block * width : (block + 1) * width] * (
                1.0 + vectors[block, scale_row : scale_row + 1, :]
            )
            moved = values * inverse * factor + vectors[block, shift_row : shift_row + 1, :]
            store(read, block * width, rounded(moved))


def context_kernel(context, vectors, gain, key_weight, value_weight, out, hidden):
    def store(_, column, rows):
        hidden[:, column : column + rows.shape[1]] = rows

    modulated([lambda c, n: context[:, c : c + n].astype(jnp.float32)], vectors, gain, 1, 3, store)
    weight = jnp.concatenate([key_weight[...], value_weight[...]], axis=0)
    pair = rounded(contract(hidden[...], weight, 1))
    for copy in range(out.shape[0]):
        out[copy] = pair


def turned(values, cosine, sine):
    lane = lax.broadcasted_iota(jnp.int32, values.shape, 1)
    half = HEAD_SIZE // 2
    other = jnp.where(
        lane % HEAD_SIZE < half, pltpu.roll(values, LANES - half, 1), pltpu.roll(values, half, 1)
    )
    return values * cosine + other * sine


def key_kernel(*refs, pieces, per_group):
    count = sum(len(piece) for piece in pieces)
    blocks = list(refs[:count])
    vectors, gain, key_weight, value_weight, cosine, sine = refs[count : 6 + count]
    hidden, key_value, first, last, ordered = refs[6 + count :]
    own = hidden.shape[0] // len(pieces)
    members = [[blocks.pop(0) for _ in piece] for piece in pieces]
    reads, places = [], {}
    for group in range(0, len(members), per_group):

        def read(column, columns, parts=members[group : group + per_group]):
            rows = []
            for part in parts:
                held = part[0].shape[1]
                ref, at = part[column // held], column % held
                rows.append(ref[:, at : at + columns].astype(jnp.float32))
            return jnp.concatenate(rows, axis=0) if len(rows) > 1 else rows[0]

        reads.append(read)
        places[read] = group * own

    def store(read, column, rows):
        begin = places[read]
        hidden[begin : begin + rows.shape[0], column : column + rows.shape[1]] = rows

    modulated(reads, vectors, gain, 0, 2, store)
    weight = jnp.concatenate([key_weight[...], value_weight[...]], axis=0)
    both = contract(hidden[...], weight, 1)
    lane = lax.broadcasted_iota(jnp.int32, both.shape, 1)
    both = jnp.where(lane < HEAD_SIZE, turned(both, cosine[...], sine[...]), both)
    for index, offset in enumerate(row_offsets(own, len(pieces))):
        begin = pl.multiple_of(offset, 8)
        ordered[pl.ds(begin, own), :] = both[index * own : (index + 1) * own, :]
    key_value[...] = rounded(ordered[...])
    first[...] = rounded(ordered[:WINDOW, :])
    last[...] = rounded(ordered[ordered.shape[0] - WINDOW :, :])


def query_kernel(hidden, w_query, w_gate, cosine, sine, queries, gate, held, ready, *, own):
    fetch = pltpu.make_async_copy(w_gate, held, ready)
    fetch.start()
    rows, width = hidden.shape[0], w_query.shape[1]
    projected = contract(hidden[...], w_query[...])
    heads = width // HEAD_SIZE
    lane = lax.broadcasted_iota(jnp.int32, (rows, LANES), 1)
    for pair in range(width // LANES):
        tile = turned(projected[:, pair * LANES : (pair + 1) * LANES], cosine[...], sine[...])
        tile = tile * (1.0 / math.sqrt(HEAD_SIZE))
        for odd in range(2):
            head = 2 * pair + odd
            aligned = pltpu.roll(tile, HEAD_SIZE, 1) if odd else tile
            aligned = jnp.where(lane < HEAD_SIZE, aligned, 0.0)
            for block in range(rows // own):
                begin = (block * heads + head) * own
                queries[begin : begin + own, :] = aligned[block * own : (block + 1) * own, :]
    fetch.wait()
    gate[...] = rounded(contract(hidden[...], held[...])).astype(jnp.float32)


def attend_kernel(
    sink,
    queries,
    gate,
    low,
    middle,
    high,
    ctx,
    w_out,
    out,
    padded,
    mixed,
    held,
    ready,
    *,
    own,
    span,
):
    fetch = pltpu.make_async_copy(w_out, held, ready)
    fetch.start()
    rows = middle.shape[0]
    width = w_out.shape[0]
    heads = width // HEAD_SIZE
    padded[:WINDOW, :] = low[...].astype(jnp.float32)
    padded[WINDOW : WINDOW + rows, :] = middle[...].astype(jnp.float32)
    padded[WINDOW + rows : 2 * WINDOW + rows, :] = high[...].astype(jnp.float32)
    padded[2 * WINDOW + rows :, :] = jnp.zeros_like(padded[2 * WINDOW + rows :, :])
    row = lax.broadcasted_iota(jnp.int32, (own, span), 0)
    column = lax.broadcasted_iota(jnp.int32, (own, span), 1)
    in_reach = (column >= row) & (column <= row + 2 * WINDOW)
    lane = lax.broadcasted_iota(jnp.int32, (own, LANES), 1)
    sinks = jnp.concatenate([jnp.full((own, 1), sink[h], jnp.float32) for h in range(heads)], axis=0)
    begin = lax.axis_index("sp") * rows
    total = lax.axis_size("sp") * rows
    offsets = row_offsets(own, rows // own)

    def scored(block):
        offset = pl.multiple_of(offsets[block], 8)
        keys = jnp.concatenate([rounded(padded[pl.ds(offset, span), :]), ctx[...]], axis=0)
        query = rounded(queries[block * heads * own : (block + 1) * heads * own, :])
        scores = contract(query, keys, 1)
        token = begin - WINDOW + offset + column
        seen = in_reach & (token >= 0) & (token < total)
        near = jnp.where(seen[None], scores[:, :span].reshape(heads, own, span), MASK_VALUE)
        scores = jnp.concatenate([near.reshape(heads * own, span), scores[:, span:]], axis=1)
        return scores, keys

    following = scored(0)
    for block in range(rows // own):
        scores, keys = following
        if block + 1 < rows // own:
            following = scored(block + 1)
        peak = jnp.maximum(jnp.max(scores, axis=1, keepdims=True), sinks)
        weights = jnp.exp(scores - peak)
        denominator = jnp.sum(weights, axis=1, keepdims=True) + jnp.exp(sinks - peak)
        result = contract(rounded(weights), keys) * (1.0 / denominator)
        here = slice(block * own, (block + 1) * own)
        for pair in range(heads // 2):
            even = result[2 * pair * own : (2 * pair + 1) * own, :]
            odd = result[(2 * pair + 1) * own : (2 * pair + 2) * own, :]
            attended = jnp.where(lane < HEAD_SIZE, pltpu.roll(even, HEAD_SIZE, 1), odd)
            tile = gate[here, pair * LANES : (pair + 1) * LANES]
            mixed[here, pair * LANES : (pair + 1) * LANES] = attended * (
                tile / (1.0 + jnp.exp(-tile))
            )
    fetch.wait()
    final = rounded(mixed[...])
    step = 512
    for begin in range(0, w_out.shape[1], step):
        out[:, begin : begin + step] = rounded(contract(final, held[:, begin : begin + step]))


def copy_for_each(copies, axis):
    return lax.all_to_all(copies, axis, split_axis=0, concat_axis=0, tiled=True)


def shift(block, axis, steps, wrap=True):
    count = lax.axis_size(axis)
    pairs = [(i, (i + steps) % count) for i in range(count) if wrap or 0 <= i + steps < count]
    return lax.ppermute(block, axis, pairs)


def added(first, *others):
    total = first.astype(jnp.float32)
    for other in others:
        total = total + other.astype(jnp.float32)
    return rounded(total)


def toward(block, steps):
    tp_count, dp_count = lax.axis_size("tp"), lax.axis_size("dp")
    pairs = []
    for i in range(tp_count):
        for j in range(dp_count):
            target = (i + (steps if j % 2 == 0 else -steps)) % tp_count
            pairs.append((i * dp_count + j, target * dp_count + j))
    return lax.ppermute(block, ("tp", "dp"), pairs)


def gather_rows(latent):
    back2 = toward(latent, 2)
    ahead2 = toward(latent, -2)
    back1 = toward(latent, 1)
    ahead1 = toward(latent, -1)
    far = toward(back2, 2)
    back3, ahead3 = toward(back2, 1), toward(ahead2, -1)
    return [(back3,), (back2,), (back1,), (latent,), (ahead1,), (ahead2,), (ahead3,), (far,)]


def reduce_rows(block):
    far = toward(block(4), 2)
    down3 = toward(block(-3), -1)
    up3 = toward(block(3), 1)
    minus_two = added(block(-2), down3)
    down2 = toward(minus_two, -2)
    ahead, _ = lax.optimization_barrier((block(2), minus_two))
    up2 = toward(added(ahead, up3, far), 2)
    up1 = toward(block(1), 1)
    down1 = toward(block(-1), -1)
    total = block(0).astype(jnp.float32)
    for part in (up1, down1, up2, down2):
        total = total + part.astype(jnp.float32)
    return total


def body(
    latent,
    condition,
    ctx_condition,
    context,
    mod_shift,
    mod_scale,
    mod_gate,
    norm_gain,
    w_query,
    key_weight,
    value_weight,
    w_gate,
    w_out,
    sink_logit,
):
    f32, bf16 = jnp.float32, jnp.bfloat16
    shape = jax.ShapeDtypeStruct
    sp_count, tp_count = lax.axis_size("sp"), lax.axis_size("tp")
    own, width = latent.shape
    rows = own * tp_count
    mod_rows, columns = mod_shift.shape
    behind = (tp_count - 1) // 2

    parts, cosine, sine = call(
        functools.partial(partial_kernel, own=own),
        [
            shape((sp_count, 5, columns), f32),
            shape((rows, LANES), f32),
            shape((rows, LANES), f32),
        ],
        condition,
        ctx_condition,
        mod_shift,
        mod_scale,
        mod_gate,
        specs=[HBM] * 5,
        scratch=[
            pltpu.VMEM((2, *condition.shape), f32),
            pltpu.VMEM((3, mod_rows, columns), bf16),
            pltpu.SemaphoreType.DMA((5,)),
        ],
        grant=62,
    )
    pieces = gather_rows(latent)
    parts = copy_for_each(parts, "sp")
    totals = call(total_kernel, shape((tp_count, 5, columns), f32), parts, grant=30)
    vectors = copy_for_each(totals, "tp")

    gain = norm_gain[None, :]
    kv_weights = (key_weight.T, value_weight.T)
    ctx_rows = context.shape[0]
    ctx_pair = call(
        context_kernel,
        shape((sp_count, ctx_rows, LANES), bf16),
        context,
        vectors,
        gain,
        *kv_weights,
        scratch=[pltpu.VMEM((ctx_rows, width), bf16)],
        grant=30,
    )
    ctx_all = copy_for_each(ctx_pair, "sp").reshape(sp_count * ctx_rows, LANES)

    blocks = [block for piece in pieces for block in piece]
    hidden, key_value, first, last = call(
        functools.partial(key_kernel, pieces=[[0] * len(p) for p in pieces], per_group=2),
        [
            shape((rows, width), bf16),
            shape((rows, LANES), bf16),
            shape((WINDOW, LANES), bf16),
            shape((WINDOW, LANES), bf16),
        ],
        *blocks,
        vectors,
        gain,
        *kv_weights,
        cosine,
        sine,
        scratch=[pltpu.VMEM((rows, LANES), f32)],
        grant=30,
    )
    low = shift(last, "sp", 1, wrap=False)
    high = shift(first, "sp", -1, wrap=False)
    heads = w_query.shape[1] // HEAD_SIZE
    queries, gate = call(
        functools.partial(query_kernel, own=own),
        [shape((rows * heads, LANES), f32), shape((rows, w_gate.shape[1]), f32)],
        hidden,
        w_query,
        w_gate,
        cosine,
        sine,
        specs=[VMEM, VMEM, HBM, VMEM, VMEM],
        scratch=[pltpu.VMEM(w_gate.shape, bf16), pltpu.SemaphoreType.DMA],
        flops=2 * 10**9,
        grant=46,
    )
    span = 3 * LANES
    product = call(
        functools.partial(attend_kernel, own=own, span=span),
        shape((rows, width), bf16),
        sink_logit,
        queries,
        gate,
        low,
        key_value,
        high,
        ctx_all,
        w_out,
        specs=[SMEM] + [VMEM] * 6 + [HBM],
        scratch=[
            pltpu.VMEM((rows - own + span, LANES), f32),
            pltpu.VMEM((rows, w_out.shape[0]), f32),
            pltpu.VMEM(w_out.shape, bf16),
            pltpu.SemaphoreType.DMA,
        ],
        flops=3 * 10**9,
        grant=50,
    )
    branch = reduce_rows(lambda d: product[(d + behind) * own : (d + behind + 1) * own])
    lat_gate = vectors[:, 4, :].reshape(width)
    return rounded(latent.astype(f32) + lat_gate * branch)


def solution(mesh):
    return jax.shard_map(
        body,
        mesh=mesh,
        in_specs=(
            P(("dp", "sp", "tp"), None),
            P("dp"),
            P(),
            P(("dp", "sp"), None),
            P("sp", "tp"),
            P("sp", "tp"),
            P("sp", "tp"),
            P(),
            P(None, "tp"),
            P(None, "tp"),
            P(None, "tp"),
            P(None, "tp"),
            P("tp", None),
            P("tp"),
        ),
        out_specs=P(("dp", "sp", "tp"), None),
        check_vma=False,
    )
```

```python
import functools
import math

import jax
import jax.numpy as jnp
from jax import lax
from jax.experimental import pallas as pl
from jax.experimental.pallas import tpu as pltpu
from jax.sharding import PartitionSpec as P

HEAD_SIZE = 64
WINDOW = 128
GRID_W = 64
LANES = 128
NORM_EPS = 1e-06
MASK_VALUE = -1e30
VMEM = pl.BlockSpec(memory_space=pltpu.VMEM)
HBM = pl.BlockSpec(memory_space=pltpu.HBM)
SMEM = pl.BlockSpec(memory_space=pltpu.SMEM)


def rounded(values):
    return values.astype(jnp.bfloat16)


def contract(left, right, right_dim=0):
    return lax.dot_general(
        left, right, (((1,), (right_dim,)), ((), ())), preferred_element_type=jnp.float32
    )


def call(kernel, out_shape, *operands, specs=None, scratch=(), flops=10**9, grant=30):
    return pl.pallas_call(
        kernel,
        out_shape=out_shape,
        in_specs=specs or [VMEM] * len(operands),
        out_specs=jax.tree.map(lambda _: VMEM, out_shape),
        scratch_shapes=scratch,
        compiler_params=pltpu.CompilerParams(vmem_limit_bytes=grant * 2**20),
        cost_estimate=pl.CostEstimate(flops=flops, bytes_accessed=10**6, transcendentals=0),
    )(*operands)


def row_offsets(own, count):
    direction = 1 - 2 * lax.rem(lax.axis_index("dp"), 2)
    rank = lax.axis_index("tp") + count
    behind = (count - 1) // 2
    return [
        lax.rem(rank + direction * distance, count) * own
        for distance in range(-behind, count - behind)
    ]


def partial_kernel(*refs, own):
    condition, ctx_condition, shift, scale, gate, out, cosine, sine = refs[:8]
    both, held, ready = refs[8:]
    fetches = [
        pltpu.make_async_copy(condition, both.at[0], ready.at[0]),
        pltpu.make_async_copy(ctx_condition, both.at[1], ready.at[1]),
    ]
    for index, weight in enumerate((shift, scale, gate)):
        fetches.append(pltpu.make_async_copy(weight, held.at[index], ready.at[2 + index]))
    for fetch in fetches:
        fetch.start()
    rows = cosine.shape[0]
    count = rows // own
    quarter = HEAD_SIZE // 4
    lane = lax.broadcasted_iota(jnp.int32, (own, LANES), 1)
    row = lax.broadcasted_iota(jnp.int32, (own, LANES), 0)
    entry = lane % (2 * quarter)
    inverse = jnp.exp(-math.log(10000.0) * (entry % quarter).astype(jnp.float32) / quarter)
    sign = jnp.where(lane % HEAD_SIZE < HEAD_SIZE // 2, -1.0, 1.0)
    begin = lax.axis_index("sp") * rows
    for index, offset in enumerate(row_offsets(own, count)):
        token = begin + offset + row
        angle = (
            jnp.where(entry < quarter, token // GRID_W, token % GRID_W).astype(jnp.float32)
            * inverse
        )
        cosine[index * own : (index + 1) * own, :] = jnp.cos(angle)
        sine[index * own : (index + 1) * own, :] = jnp.sin(angle) * sign
    for fetch in fetches[:2]:
        fetch.wait()
    size = held.shape[1]
    mine = pl.ds(pl.multiple_of(lax.axis_index("sp") * size, size), size)
    values = jnp.stack([both[0, mine], both[1, mine]])
    acts = rounded(values / (1.0 + jnp.exp(-values)))
    sums = []
    for index, fetch in enumerate(fetches[2:]):
        fetch.wait()
        sums.append(contract(acts, held[index]))
    sums = jnp.concatenate([sums[0], sums[1], sums[2][:1]], axis=0)
    for copy in range(out.shape[0]):
        out[copy] = sums


def total_kernel(parts, out):
    total = parts[0]
    for index in range(1, parts.shape[0]):
        total = total + parts[index]
    for copy in range(out.shape[0]):
        out[copy] = total


def modulated(pieces, vectors, gain, shift_row, scale_row, store):
    blocks, _, width = vectors.shape
    for read in pieces:
        square = None
        for block in range(blocks):
            values = read(block * width, width)
            part = sum(
                values[:, lane : lane + LANES] * values[:, lane : lane + LANES]
                for lane in range(0, width, LANES)
            )
            square = part if square is None else square + part
        mean = jnp.sum(square, axis=1, keepdims=True) / (blocks * width)
        inverse = lax.rsqrt(mean + NORM_EPS)
        for block in range(blocks):
            values = read(block * width, width)
            factor = gain[:, block * width : (block + 1) * width] * (
                1.0 + vectors[block, scale_row : scale_row + 1, :]
            )
            moved = values * inverse * factor + vectors[block, shift_row : shift_row + 1, :]
            store(read, block * width, rounded(moved))


def context_kernel(context, vectors, gain, key_weight, value_weight, out, hidden):
    def store(_, column, rows):
        hidden[:, column : column + rows.shape[1]] = rows

    modulated([lambda c, n: context[:, c : c + n].astype(jnp.float32)], vectors, gain, 1, 3, store)
    weight = jnp.concatenate([key_weight[...], value_weight[...]], axis=0)
    pair = rounded(contract(hidden[...], weight, 1))
    for copy in range(out.shape[0]):
        out[copy] = pair


def turned(values, cosine, sine):
    lane = lax.broadcasted_iota(jnp.int32, values.shape, 1)
    half = HEAD_SIZE // 2
    other = jnp.where(
        lane % HEAD_SIZE < half, pltpu.roll(values, LANES - half, 1), pltpu.roll(values, half, 1)
    )
    return values * cosine + other * sine


def key_kernel(*refs, pieces, per_group):
    count = sum(len(piece) for piece in pieces)
    blocks = list(refs[:count])
    vectors, gain, key_weight, value_weight, cosine, sine = refs[count : 6 + count]
    hidden, key_value, first, last, ordered = refs[6 + count :]
    own = hidden.shape[0] // len(pieces)
    members = [[blocks.pop(0) for _ in piece] for piece in pieces]
    reads, places = [], {}
    for group in range(0, len(members), per_group):

        def read(column, columns, parts=members[group : group + per_group]):
            rows = []
            for part in parts:
                held = part[0].shape[1]
                ref, at = part[column // held], column % held
                rows.append(ref[:, at : at + columns].astype(jnp.float32))
            return jnp.concatenate(rows, axis=0) if len(rows) > 1 else rows[0]

        reads.append(read)
        places[read] = group * own

    def store(read, column, rows):
        begin = places[read]
        hidden[begin : begin + rows.shape[0], column : column + rows.shape[1]] = rows

    modulated(reads, vectors, gain, 0, 2, store)
    weight = jnp.concatenate([key_weight[...], value_weight[...]], axis=0)
    both = contract(hidden[...], weight, 1)
    lane = lax.broadcasted_iota(jnp.int32, both.shape, 1)
    both = jnp.where(lane < HEAD_SIZE, turned(both, cosine[...], sine[...]), both)
    for index, offset in enumerate(row_offsets(own, len(pieces))):
        begin = pl.multiple_of(offset, 8)
        ordered[pl.ds(begin, own), :] = both[index * own : (index + 1) * own, :]
    key_value[...] = rounded(ordered[...])
    first[...] = rounded(ordered[:WINDOW, :])
    last[...] = rounded(ordered[ordered.shape[0] - WINDOW :, :])


def query_kernel(hidden, w_query, w_gate, cosine, sine, queries, gate, held, ready, *, own):
    fetch = pltpu.make_async_copy(w_gate, held, ready)
    fetch.start()
    rows, width = hidden.shape[0], w_query.shape[1]
    projected = contract(hidden[...], w_query[...])
    heads = width // HEAD_SIZE
    lane = lax.broadcasted_iota(jnp.int32, (rows, LANES), 1)
    for pair in range(width // LANES):
        tile = turned(projected[:, pair * LANES : (pair + 1) * LANES], cosine[...], sine[...])
        tile = tile * (1.0 / math.sqrt(HEAD_SIZE))
        for odd in range(2):
            head = 2 * pair + odd
            aligned = pltpu.roll(tile, HEAD_SIZE, 1) if odd else tile
            aligned = jnp.where(lane < HEAD_SIZE, aligned, 0.0)
            for block in range(rows // own):
                begin = (block * heads + head) * own
                queries[begin : begin + own, :] = aligned[block * own : (block + 1) * own, :]
    fetch.wait()
    gate[...] = rounded(contract(hidden[...], held[...])).astype(jnp.float32)


def attend_kernel(
    sink,
    queries,
    gate,
    low,
    middle,
    high,
    ctx,
    w_out,
    out,
    padded,
    mixed,
    held,
    ready,
    *,
    own,
    span,
    served,
):
    fetch = pltpu.make_async_copy(w_out, held, ready)
    fetch.start()
    rows = middle.shape[0]
    width = w_out.shape[0]
    heads = width // HEAD_SIZE
    padded[:WINDOW, :] = low[...].astype(jnp.float32)
    padded[WINDOW : WINDOW + rows, :] = middle[...].astype(jnp.float32)
    padded[WINDOW + rows : 2 * WINDOW + rows, :] = high[...].astype(jnp.float32)
    padded[2 * WINDOW + rows :, :] = jnp.zeros_like(padded[2 * WINDOW + rows :, :])
    row = lax.broadcasted_iota(jnp.int32, (own, span), 0)
    column = lax.broadcasted_iota(jnp.int32, (own, span), 1)
    in_reach = (column >= row) & (column <= row + 2 * WINDOW)
    lane = lax.broadcasted_iota(jnp.int32, (own, LANES), 1)
    sinks = jnp.concatenate([jnp.full((own, 1), sink[h], jnp.float32) for h in range(heads)], axis=0)
    begin = lax.axis_index("sp") * rows
    total = lax.axis_size("sp") * rows
    offsets = row_offsets(own, rows // own)

    def scored(block):
        offset = pl.multiple_of(offsets[block], 8)
        keys = jnp.concatenate([rounded(padded[pl.ds(offset, span), :]), ctx[...]], axis=0)
        query = rounded(queries[block * heads * own : (block + 1) * heads * own, :])
        scores = contract(query, keys, 1)
        token = begin - WINDOW + offset + column
        seen = in_reach & (token >= 0) & (token < total)
        near = jnp.where(seen[None], scores[:, :span].reshape(heads, own, span), MASK_VALUE)
        scores = jnp.concatenate([near.reshape(heads * own, span), scores[:, span:]], axis=1)
        return scores, keys

    following = scored(served[0])
    for at, block in enumerate(served):
        scores, keys = following
        if at + 1 < len(served):
            following = scored(served[at + 1])
        peak = jnp.maximum(jnp.max(scores, axis=1, keepdims=True), sinks)
        weights = jnp.exp(scores - peak)
        denominator = jnp.sum(weights, axis=1, keepdims=True) + jnp.exp(sinks - peak)
        result = contract(rounded(weights), keys) * (1.0 / denominator)
        here = slice(block * own, (block + 1) * own)
        for pair in range(heads // 2):
            even = result[2 * pair * own : (2 * pair + 1) * own, :]
            odd = result[(2 * pair + 1) * own : (2 * pair + 2) * own, :]
            attended = jnp.where(lane < HEAD_SIZE, pltpu.roll(even, HEAD_SIZE, 1), odd)
            tile = gate[here, pair * LANES : (pair + 1) * LANES]
            mixed[at * own : (at + 1) * own, pair * LANES : (pair + 1) * LANES] = attended * (
                tile / (1.0 + jnp.exp(-tile))
            )
    fetch.wait()
    final = rounded(mixed[...])
    step = 512
    for begin in range(0, w_out.shape[1], step):
        out[:, begin : begin + step] = rounded(contract(final, held[:, begin : begin + step]))


def copy_for_each(copies, axis):
    return lax.all_to_all(copies, axis, split_axis=0, concat_axis=0, tiled=True)


def shift(block, axis, steps, wrap=True):
    count = lax.axis_size(axis)
    pairs = [(i, (i + steps) % count) for i in range(count) if wrap or 0 <= i + steps < count]
    return lax.ppermute(block, axis, pairs)


def added(first, *others):
    total = first.astype(jnp.float32)
    for other in others:
        total = total + other.astype(jnp.float32)
    return rounded(total)


def toward(block, steps):
    tp_count, dp_count = lax.axis_size("tp"), lax.axis_size("dp")
    pairs = []
    for i in range(tp_count):
        for j in range(dp_count):
            target = (i + (steps if j % 2 == 0 else -steps)) % tp_count
            pairs.append((i * dp_count + j, target * dp_count + j))
    return lax.ppermute(block, ("tp", "dp"), pairs)


def gather_rows(latent):
    back2 = toward(latent, 2)
    ahead2 = toward(latent, -2)
    back1 = toward(latent, 1)
    ahead1 = toward(latent, -1)
    far = toward(back2, 2)
    back3, ahead3 = toward(back2, 1), toward(ahead2, -1)
    return [(back3,), (back2,), (back1,), (latent,), (ahead1,), (ahead2,), (ahead3,), (far,)]


def reduce_rows(block):
    far = toward(block(4), 2)
    down3 = toward(block(-3), -1)
    up3 = toward(block(3), 1)
    minus_two = added(block(-2), down3)
    down2 = toward(minus_two, -2)
    ahead, _ = lax.optimization_barrier((block(2), minus_two))
    up2 = toward(added(ahead, up3, far), 2)
    up1 = toward(block(1), 1)
    down1 = toward(block(-1), -1)
    total = block(0).astype(jnp.float32)
    for part in (up1, down1, up2, down2):
        total = total + part.astype(jnp.float32)
    return total


def body(
    latent,
    condition,
    ctx_condition,
    context,
    mod_shift,
    mod_scale,
    mod_gate,
    norm_gain,
    w_query,
    key_weight,
    value_weight,
    w_gate,
    w_out,
    sink_logit,
):
    f32, bf16 = jnp.float32, jnp.bfloat16
    shape = jax.ShapeDtypeStruct
    sp_count, tp_count = lax.axis_size("sp"), lax.axis_size("tp")
    own, width = latent.shape
    rows = own * tp_count
    mod_rows, columns = mod_shift.shape
    behind = (tp_count - 1) // 2

    parts, cosine, sine = call(
        functools.partial(partial_kernel, own=own),
        [
            shape((sp_count, 5, columns), f32),
            shape((rows, LANES), f32),
            shape((rows, LANES), f32),
        ],
        condition,
        ctx_condition,
        mod_shift,
        mod_scale,
        mod_gate,
        specs=[HBM] * 5,
        scratch=[
            pltpu.VMEM((2, *condition.shape), f32),
            pltpu.VMEM((3, mod_rows, columns), bf16),
            pltpu.SemaphoreType.DMA((5,)),
        ],
        grant=62,
    )
    pieces = gather_rows(latent)
    parts = copy_for_each(parts, "sp")
    totals = call(total_kernel, shape((tp_count, 5, columns), f32), parts, grant=30)
    vectors = copy_for_each(totals, "tp")

    gain = norm_gain[None, :]
    kv_weights = (key_weight.T, value_weight.T)
    ctx_rows = context.shape[0]
    ctx_pair = call(
        context_kernel,
        shape((sp_count, ctx_rows, LANES), bf16),
        context,
        vectors,
        gain,
        *kv_weights,
        scratch=[pltpu.VMEM((ctx_rows, width), bf16)],
        grant=30,
    )
    ctx_all = copy_for_each(ctx_pair, "sp").reshape(sp_count * ctx_rows, LANES)

    blocks = [block for piece in pieces for block in piece]
    hidden, key_value, first, last = call(
        functools.partial(key_kernel, pieces=[[0] * len(p) for p in pieces], per_group=2),
        [
            shape((rows, width), bf16),
            shape((rows, LANES), bf16),
            shape((WINDOW, LANES), bf16),
            shape((WINDOW, LANES), bf16),
        ],
        *blocks,
        vectors,
        gain,
        *kv_weights,
        cosine,
        sine,
        scratch=[pltpu.VMEM((rows, LANES), f32)],
        grant=30,
    )
    low = shift(last, "sp", 1, wrap=False)
    high = shift(first, "sp", -1, wrap=False)
    heads = w_query.shape[1] // HEAD_SIZE
    queries, gate = call(
        functools.partial(query_kernel, own=own),
        [shape((rows * heads, LANES), f32), shape((rows, w_gate.shape[1]), f32)],
        hidden,
        w_query,
        w_gate,
        cosine,
        sine,
        specs=[VMEM, VMEM, HBM, VMEM, VMEM],
        scratch=[pltpu.VMEM(w_gate.shape, bf16), pltpu.SemaphoreType.DMA],
        flops=2 * 10**9,
        grant=46,
    )
    span = 3 * LANES

    def attend(distances):
        served = tuple(distance + behind for distance in distances)
        product = call(
            functools.partial(attend_kernel, own=own, span=span, served=served),
            shape((own * len(served), width), bf16),
            sink_logit,
            queries,
            gate,
            low,
            key_value,
            high,
            ctx_all,
            w_out,
            specs=[SMEM] + [VMEM] * 6 + [HBM],
            scratch=[
                pltpu.VMEM((rows - own + span, LANES), f32),
                pltpu.VMEM((own * len(served), w_out.shape[0]), f32),
                pltpu.VMEM(w_out.shape, bf16),
                pltpu.SemaphoreType.DMA,
            ],
            flops=10**9,
            grant=50,
        )
        return {
            distance: product[at * own : (at + 1) * own] for at, distance in enumerate(distances)
        }

    product = attend((4, -3, 3))
    product.update(attend((-2, 2, 1, 0, -1)))
    branch = reduce_rows(product.__getitem__)
    lat_gate = vectors[:, 4, :].reshape(width)
    return rounded(latent.astype(f32) + lat_gate * branch)


def solution(mesh):
    return jax.shard_map(
        body,
        mesh=mesh,
        in_specs=(
            P(("dp", "sp", "tp"), None),
            P("dp"),
            P(),
            P(("dp", "sp"), None),
            P("sp", "tp"),
            P("sp", "tp"),
            P("sp", "tp"),
            P(),
            P(None, "tp"),
            P(None, "tp"),
            P(None, "tp"),
            P(None, "tp"),
            P("tp", None),
            P("tp"),
        ),
        out_specs=P(("dp", "sp", "tp"), None),
        check_vma=False,
    )
```
